32 devices in a mesh: sp: 16 (over z, x, core), tp: 2 (over y).
Axes of the slice: x: 2, y: 2, z: 4, core: 2. Of those that a mesh axis runs over, the one named last changes fastest.
Arguments:
- residual: bfloat16 [4096, 2048], P(('sp', 'tp')), may hold values from -6 to 6
- query_vectors: bfloat16 [4096, 512], P('sp', 'tp'), may hold values from -6 to 6
- key_vectors: bfloat16 [4096, 512], P('sp', 'tp'), may hold values from -6 to 6
- value_vectors: bfloat16 [4096, 512], P('sp', 'tp'), may hold values from -6 to 6
- in_gate: float32 [8, 4096], P('tp', 'sp'), may hold values from -9 to 190
- forget_gate: float32 [8, 4096], P('tp', 'sp'), may hold values from -1 to 12
- documents: int32 [4096], P('sp'), may hold values from 0 to 3, never falling along the last dimension, each value on 1 to 2048 neighbouring positions
- w_out: bfloat16 [512, 2048], P('tp'), may hold values from -0.25 to 0.25
- norm_gain: bfloat16 [2048], replicated, may hold values from 0.099609375 to 1.8984375
- w_up: bfloat16 [2048, 8192], P('sp', 'tp'), may hold values from -0.125 to 0.125
- w_down: bfloat16 [8192, 2048], P('tp', 'sp'), may hold values from -0.0625 to 0.0625
Outputs:
- layer_out: bfloat16 [4096, 2048], P(('sp', 'tp'))
The draws below stay inside these ranges and needn't reach their ends.
Inputs may be any that keep to these rules, and one draw needn't show every extreme that they name: `documents`: document numbers never fall along the positions; every document has 1 to 2048 positions.
All inputs are finite; a program needn't handle non-finite values.
Results may differ from the reference program's by a relative error of at most 0.015.
Values may be sent and summed in bfloat16 or wider, within the bound.
A program may use at most 128 MiB of HBM per device.

```python
import math
import jax
import jax.numpy as jnp
import numpy as np
from jax import lax

D = 2048
MEMORY_HEADS = 8
FF = 8192
SPAN = 128
TOK_DEV = 256
HW = 512
PACKED_TOKENS = 4096
DOCS = 4
DOC_MOST = 2048
N_TP = 2


def draw_in_gate(key, part):
    base_key = jax.random.fold_in(key, 0)
    drawn = jnp.clip(jax.random.normal(base_key, (MEMORY_HEADS, PACKED_TOKENS), jnp.float32), -5.5, 4.5) - 3.5
    return drawn


def draw_forget_gate(key, part):
    shuffle_random_key, gradual_random_key, quick_random_key, block_random_key, jitter_random_key, spike_random_key, dropout_random_key = jax.random.split(key, 7)
    head_order = jax.random.permutation(shuffle_random_key, MEMORY_HEADS)
    slow_count = MEMORY_HEADS // 2
    slow_heads = head_order < slow_count
    slow_rate = math.log(10.0) / DOC_MOST * jax.random.uniform(gradual_random_key, (MEMORY_HEADS,), jnp.float32, 0.3, 1.0)
    fast_rate = 1.0 / jax.random.uniform(quick_random_key, (MEMORY_HEADS,), jnp.float32, 30.0, 100.0)
    head_rate = jnp.where(slow_heads, slow_rate, fast_rate)
    block_factor = jnp.exp(jax.random.uniform(block_random_key, (PACKED_TOKENS // TOK_DEV,), jnp.float32, 0.0, math.log(3.0)))
    position_factor = jnp.repeat(block_factor, TOK_DEV)
    noise_part = jax.random.uniform(jitter_random_key, (MEMORY_HEADS, PACKED_TOKENS), jnp.float32, -1.0, 1.0)
    step_rate = head_rate[:, None] * position_factor[None, :] * jnp.exp(noise_part)
    gate_logits = -jnp.log(jnp.expm1(step_rate))
    spike_positions = jax.random.randint(spike_random_key, (4,), 0, PACKED_TOKENS)
    spike_mask = jnp.any(jnp.arange(PACKED_TOKENS)[:, None] == spike_positions[None, :], axis=1)
    spike_height = jax.random.uniform(dropout_random_key, (MEMORY_HEADS, PACKED_TOKENS), jnp.float32, -0.4, 1.4)
    return jnp.where(spike_mask[None, :], spike_height, gate_logits)


def shard_levels(key, shape, cuts, least, largest):
    level = 1.0
    for position, shards_of in cuts:
        heights = jax.random.uniform(jax.random.fold_in(jax.random.fold_in(key, 6), position), (shards_of,), jnp.float32, least / len(cuts), largest / len(cuts))
        level = level * jnp.repeat(jnp.exp(heights), shape[position] // shards_of).reshape((-1,) + (1,) * (len(shape) - 1 - position))
    return level


def length_profile(amount, total, limit, skew):
    loads = [(1 << 20) // math.isqrt(rank ** skew) + 1 for rank in range(2, amount + 1)]
    rest, given = total - limit - (amount - 1), [1] * (amount - 1)
    while rest > 0:
        free = [i for i in range(amount - 1) if given[i] < limit]
        pool, remaining = sum([loads[i] for i in free]), rest
        for i in free:
            more = min(limit - given[i], max(1, remaining * loads[i] // pool), rest)
            given[i] = given[i] + more
            rest = rest - more
    return np.array([limit] + given)


def ragged_sizes(own_key, count, total, most, lean):
    if count == 2:
        one = jax.random.randint(own_key, (), max(1, total - most), min(most, total - 1) + 1)
        return jnp.stack([one, total - one])
    lengths = jnp.asarray(length_profile(count, total, most, lean), jnp.int32)
    twos = (count - 1) // 2
    donor, receiver = lengths[1:1 + 2 * twos:2], lengths[2:2 + 2 * twos:2]
    margin = jnp.minimum(donor - 1, most - receiver)
    moved = jax.random.randint(jax.random.fold_in(own_key, 1), (twos,), 0, 1 << 20) % (margin + 1)
    lengths = lengths.at[1:1 + 2 * twos:2].set(donor - moved).at[2:2 + 2 * twos:2].set(receiver + moved)
    return lengths[jax.random.permutation(jax.random.fold_in(own_key, 2), count)]


def gaussian(rng, dims, width, most, pieces=(), held_as=jnp.bfloat16):
    values = width * jax.random.normal(rng, dims, jnp.float32)
    if pieces:
        values = values * shard_levels(rng, dims, pieces, -0.22, 0.18)
    return jnp.clip(values, -most, most).astype(held_as)


def setup_inputs(seed: int = 0) -> dict:
    arg_keys = jax.random.split(jax.random.key(seed), 12)
    residual = gaussian(arg_keys[0], (PACKED_TOKENS, D), 1.0, 6.0, ((0, 32),))
    query_vectors = gaussian(arg_keys[1], (PACKED_TOKENS, HW), 1.0, 6.0, ((0, 16), (1, 2)))
    key_vectors = gaussian(arg_keys[2], (PACKED_TOKENS, HW), 1.0, 6.0, ((0, 16), (1, 2)))
    value_vectors = gaussian(arg_keys[3], (PACKED_TOKENS, HW), 1.0, 6.0, ((0, 16), (1, 2)))
    in_gate = draw_in_gate(jax.random.fold_in(arg_keys[11], 71), 0)
    forget_gate = draw_forget_gate(jax.random.fold_in(arg_keys[11], 71), 0)
    documents = jnp.searchsorted(jnp.cumsum(ragged_sizes(arg_keys[6], DOCS, PACKED_TOKENS, DOC_MOST, 0)), jnp.arange(PACKED_TOKENS), side="right").astype(jnp.int32)
    w_out = gaussian(arg_keys[7], (HW, D), HW ** -0.5, 0.25, ((0, 2),))
    norm_gain = jnp.clip(1.0 + 0.18 * jax.random.normal(arg_keys[8], (D,), jnp.float32), 0.099609375, 1.8984375).astype(jnp.bfloat16)
    w_up = gaussian(arg_keys[9], (D, FF), D ** -0.5, 0.125, ((0, 16), (1, 2)))
    w_down = gaussian(arg_keys[10], (FF, D), FF ** -0.5, 0.0625, ((0, 2), (1, 16)))
    return {"residual": residual, "query_vectors": query_vectors, "key_vectors": key_vectors, "value_vectors": value_vectors, "in_gate": in_gate, "forget_gate": forget_gate, "documents": documents, "w_out": w_out, "norm_gain": norm_gain, "w_up": w_up, "w_down": w_down}


very_negative = -1e+30
epsilon = 1e-06

def identity_state(head_count, head_dim):
    return (jnp.zeros((head_count, head_dim, head_dim), jnp.float32), jnp.zeros((head_count, head_dim), jnp.float32), jnp.full((head_count,), very_negative, jnp.float32), jnp.zeros((head_count,), jnp.float32), jnp.array(-1.0, jnp.float32), jnp.array(-1.0, jnp.float32))

def combine(earlier, later):
    memory_one, normal_one, top_one, decay_one, first_one, last_one = earlier
    memory_two, normal_two, top_two, decay_two, first_two, last_two = later
    later_empty = first_two < 0.0
    earlier_empty = first_one < 0.0
    keep = later_empty | (first_two == last_two) & (first_two == last_one)
    decay_step = jnp.where(later_empty, 0.0, decay_two)
    top_new = jnp.where(keep, jnp.maximum(decay_step + top_one, top_two), top_two)
    scale_old = jnp.where(keep, jnp.exp(decay_step + top_one - top_new), 0.0)
    scale_new = jnp.exp(top_two - top_new)
    memory_new = scale_old[:, None, None] * memory_one + scale_new[:, None, None] * memory_two
    normal_new = scale_old[:, None] * normal_one + scale_new[:, None] * normal_two
    decay_new = jnp.where(keep, decay_one + decay_step, decay_two)
    first_new = jnp.where(earlier_empty, first_two, first_one)
    last_new = jnp.where(later_empty, last_one, last_two)
    return (memory_new, normal_new, top_new, decay_new, first_new, last_new)

def block_summary(key_block, value_block, gate_block, decay_block, segment):
    cumulative = jnp.cumsum(decay_block, axis=-1)
    latest = segment == segment[-1]
    growth = jnp.where(latest[None, :], cumulative[:, -1:] - cumulative + gate_block, very_negative)
    top_log = lax.optimization_barrier(jnp.max(growth, axis=-1))
    weight_table = jnp.exp(growth - top_log[:, None])
    key_expanded = key_block.astype(jnp.float32)
    value_expanded = value_block.astype(jnp.float32)
    memory_matrix = jnp.einsum('jw,wjm,wju->jmu', weight_table, key_expanded, value_expanded, precision=lax.Precision.HIGHEST)
    normal = jnp.einsum('hs,shk->hk', weight_table, key_expanded, precision=lax.Precision.HIGHEST)
    return (memory_matrix, normal, top_log, cumulative[:, -1], segment[0], segment[-1])

def block_output(query_block, key_block, value_block, gate_block, decay_block, segment, state):
    memory_matrix, normal, top_log, total_decay, first_doc, last_doc = state
    head_dim = query_block.shape[2]
    length = segment.shape[0]
    cumulative = jnp.cumsum(decay_block, axis=-1)
    row_ids = lax.broadcasted_iota(jnp.int32, (length, length), 0)
    col_ids = lax.broadcasted_iota(jnp.int32, (length, length), 1)
    allowed = (col_ids <= row_ids) & (segment[:, None] == segment[None, :])
    inside = jnp.where(allowed[None], cumulative[:, :, None] - cumulative[:, None, :] + gate_block[:, None, :], very_negative)
    outside = jnp.where((segment == last_doc)[None, :], cumulative + top_log[:, None], very_negative)
    peak_log = jnp.maximum(outside, lax.optimization_barrier(jnp.max(inside, axis=-1)))
    carried = jnp.exp(outside - peak_log)
    scaled_expanded = query_block.astype(jnp.float32) * head_dim ** (-0.5)
    scores = jnp.einsum('lhd,shd->hls', scaled_expanded, key_block.astype(jnp.float32))
    weight_table = jnp.exp(inside - peak_log[:, :, None]) * scores
    rounded = lax.optimization_barrier(weight_table.astype(jnp.bfloat16))
    from_block = jnp.einsum('hls,shv->hlv', rounded.astype(jnp.float32), value_block.astype(jnp.float32))
    memory_readout = jnp.einsum('pug,uga->upa', scaled_expanded, memory_matrix, precision=lax.Precision.HIGHEST)
    numer_part = carried[:, :, None] * memory_readout + from_block
    denom_part = carried * jnp.einsum('lhk,hk->hl', scaled_expanded, normal, precision=lax.Precision.HIGHEST) + lax.optimization_barrier(jnp.sum(weight_table, axis=-1))
    result = numer_part / jnp.maximum(jnp.abs(denom_part), jnp.exp(-peak_log))[:, :, None]
    return jnp.transpose(result, (1, 0, 2)).reshape(length, -1).astype(jnp.bfloat16)

def reference(residual, query_vectors, key_vectors, value_vectors, in_gate, forget_gate, documents, w_out, norm_gain, w_up, w_down):
    head_count = in_gate.shape[0]
    head_dim = query_vectors.shape[1] // head_count
    total_rows = query_vectors.shape[0]
    block_count = total_rows // SPAN

    def to_blocks(vectors):
        return vectors.reshape(block_count, SPAN, head_count, head_dim)

    def gate_blocks(gates):
        return jnp.transpose(gates.reshape(head_count, block_count, SPAN), (1, 0, 2))
    segments = documents.astype(jnp.float32).reshape(block_count, SPAN)
    inputs_all = (to_blocks(query_vectors), to_blocks(key_vectors), to_blocks(value_vectors), gate_blocks(in_gate), gate_blocks(jax.nn.log_sigmoid(forget_gate)), segments)

    def block_step(state, inputs):
        query_block, key_block, value_block, gate_block, decay_block, segment = inputs
        output = block_output(query_block, key_block, value_block, gate_block, decay_block, segment, state)
        summary = block_summary(key_block, value_block, gate_block, decay_block, segment)
        return (combine(state, summary), output)
    _, mixed = lax.scan(block_step, identity_state(head_count, head_dim), inputs_all)
    mixed = mixed.reshape(total_rows, head_count * head_dim)
    group_width = w_up.shape[1] // N_TP

    def row_block(inputs):
        mixed_rows, residual_rows = inputs
        projected = jnp.dot(mixed_rows, w_out, preferred_element_type=jnp.float32)
        middle = (residual_rows.astype(jnp.float32) + projected).astype(jnp.bfloat16)
        middle_wide = middle.astype(jnp.float32)
        factor = lax.rsqrt(lax.optimization_barrier(jnp.mean(middle_wide * middle_wide, axis=-1, keepdims=True)) + epsilon)
        normed = (middle_wide * factor * norm_gain.astype(jnp.float32)).astype(jnp.bfloat16)
        lifted = jnp.dot(normed, w_up, preferred_element_type=jnp.float32)
        hidden = jnp.square(jax.nn.relu(lifted)).astype(jnp.bfloat16)
        summed = jnp.zeros(middle.shape, jnp.float32)
        for column_group in range(N_TP):
            lower = column_group * group_width
            partial_sum = jnp.dot(hidden[:, lower:lower + group_width], w_down[lower:lower + group_width], preferred_element_type=jnp.float32)
            rounded = lax.optimization_barrier(partial_sum.astype(jnp.bfloat16))
            summed = summed + rounded.astype(jnp.float32)
        return (middle_wide + summed).astype(jnp.bfloat16)
    blocks_out = lax.map(row_block, (mixed.reshape(-1, TOK_DEV, head_count * head_dim), residual.reshape(-1, TOK_DEV, residual.shape[1])))
    return blocks_out.reshape(residual.shape)
```

```python
import functools

import jax
import jax.numpy as jnp
import numpy as np
from jax import lax
from jax.experimental import pallas as pl
from jax.experimental.pallas import tpu as pltpu
from jax.sharding import Mesh, PartitionSpec as P

DOC_MOST = 2048
very_negative = -1e30
epsilon = 1e-06
SP = ("z", "x", "c")
G = ("x", "c")


def combine(earlier, later):
    memory_one, top_one, decay_one, first_one, last_one = earlier
    memory_two, top_two, decay_two, first_two, last_two = later
    later_empty = first_two < 0.0
    earlier_empty = first_one < 0.0
    keep = later_empty | (first_two == last_two) & (first_two == last_one)
    decay_step = jnp.where(later_empty, 0.0, decay_two)
    top_new = jnp.where(keep, jnp.maximum(decay_step + top_one, top_two), top_two)
    scale_old = jnp.where(keep, jnp.exp(decay_step + top_one - top_new), 0.0)
    scale_new = jnp.exp(top_two - top_new)
    memory_new = scale_old[:, None, None] * memory_one + scale_new[:, None, None] * memory_two
    decay_new = jnp.where(keep, decay_one + decay_step, decay_two)
    first_new = jnp.where(earlier_empty, first_two, first_one)
    last_new = jnp.where(later_empty, last_one, last_two)
    return (memory_new, top_new, decay_new, first_new, last_new)


def pack(state):
    memory, top, decay, first, last = state
    heads, _, width = memory.shape
    row = jnp.stack(
        [top, decay, jnp.broadcast_to(first, top.shape), jnp.broadcast_to(last, top.shape)], axis=1
    )
    row = jnp.pad(row, ((0, 0), (0, width - 4)))
    return jnp.concatenate(
        [memory, row[:, None, :], jnp.zeros((heads, 6, width), jnp.float32)], axis=1
    )


def unpack(packed, present):
    rows = packed.shape[1] - 7
    row = packed[:, rows]
    memory = jnp.where(present, packed[:, :rows], 0.0)
    top = jnp.where(present, row[:, 0], very_negative)
    decay = jnp.where(present, row[:, 1], 0.0)
    first = jnp.where(present, row[0, 2], -1.0)
    last = jnp.where(present, row[0, 3], -1.0)
    return (memory, top, decay, first, last)


def shifted(state, distance, length, here):
    packed = lax.ppermute(pack(state), SP, [(i, i + distance) for i in range(length - distance)])
    return unpack(packed, here >= distance)


def turn(value, axis, d):
    n = lax.axis_size(axis)
    return lax.ppermute(value, axis, [(i, (i + d) % n) for i in range(n)])


def reduced(terms, dim, axis):
    def block(d):
        return lax.index_in_dim(terms, d, dim, keepdims=False)

    total = block(0).astype(jnp.float32)
    for d in range(1, lax.axis_size(axis)):
        total = total + turn(block(d), axis, -d).astype(jnp.float32)
    return total.astype(jnp.bfloat16)


def on_device(
    residual,
    query_vectors,
    key_vectors,
    value_vectors,
    in_gate,
    forget_gate,
    documents,
    w_out,
    norm_gain,
    w_up,
    w_down,
):
    tok_rows = query_vectors.shape[0]
    heads = in_gate.shape[0]
    head_dim = query_vectors.shape[1] // heads
    length = lax.axis_size(SP)
    here = lax.axis_index(SP)
    tp = lax.axis_size("tp")
    me = lax.axis_index("tp")

    plane = lax.axis_size(G)
    up_pieces = jnp.transpose(w_up.reshape(w_up.shape[0], plane, -1), (1, 0, 2))
    up_part = lax.all_to_all(up_pieces, G, split_axis=0, concat_axis=0, tiled=True)
    up_part = up_part.reshape(-1, up_part.shape[-1])
    up_part, w_down, w_out, key_vectors, in_gate, forget_gate, documents = (
        lax.optimization_barrier(
            (up_part, w_down, w_out, key_vectors, in_gate, forget_gate, documents)
        )
    )
    down_part = lax.all_to_all(w_down, G, split_axis=0, concat_axis=1, tiled=True)
    up_all = lax.all_gather(up_part, "z", axis=0, tiled=True)
    down_all = lax.all_gather(down_part, "z", axis=1, tiled=True)

    w_out_parts = [w_out] + [turn(w_out, "tp", d) for d in range(1, tp)]

    segment = documents.astype(jnp.float32)
    decay_log = jax.nn.log_sigmoid(forget_gate)
    cumulative = jnp.cumsum(decay_log, axis=-1)
    key_heads = jnp.transpose(key_vectors.reshape(tok_rows, heads, head_dim), (1, 0, 2))
    value_heads = jnp.transpose(value_vectors.reshape(tok_rows, heads, head_dim), (1, 0, 2))
    query_heads = jnp.transpose(query_vectors.reshape(tok_rows, heads, head_dim), (1, 0, 2))
    query_heads = query_heads * jnp.asarray(head_dim ** (-0.5), query_heads.dtype)
    latest = segment == segment[-1]
    growth = jnp.where(latest[None, :], cumulative[:, -1:] - cumulative + in_gate, very_negative)
    top_log = jnp.max(growth, axis=-1)
    summary_weight = jnp.exp(growth - top_log[:, None])
    key_wide = key_heads.astype(jnp.float32)
    weighted = key_wide * summary_weight[:, :, None]
    memory = jnp.einsum(
        "hsv,hsk->hvk", value_heads.astype(jnp.float32), weighted, precision=lax.Precision.HIGHEST
    )
    normal = jnp.sum(weighted, axis=1)
    state = (
        jnp.concatenate([memory, normal[:, None, :]], axis=1),
        top_log,
        cumulative[:, -1],
        segment[0],
        segment[-1],
    )

    reach = min(length - 1, -(-(DOC_MOST - 1) // tok_rows))
    span = 1
    while span < reach:
        state = combine(shifted(state, span, length, here), state)
        span *= 2
    incoming = shifted(state, 1, length, here)
    memory_in, top_in, _, _, last_in = incoming

    row_ids = lax.broadcasted_iota(jnp.int32, (tok_rows, tok_rows), 0)
    col_ids = lax.broadcasted_iota(jnp.int32, (tok_rows, tok_rows), 1)
    allowed = (col_ids <= row_ids) & (segment[:, None] == segment[None, :])
    inside = jnp.where(
        allowed[None],
        cumulative[:, :, None] - cumulative[:, None, :] + in_gate[:, None, :],
        very_negative,
    )
    peak_inside = jnp.max(inside, axis=-1)
    scores = jnp.einsum(
        "hld,hsd->hls", query_heads, key_heads, preferred_element_type=jnp.float32
    )
    weight_inside = jnp.exp(inside - peak_inside[:, :, None]) * scores
    from_block = jnp.einsum(
        "hls,hsv->hlv",
        weight_inside.astype(jnp.bfloat16),
        value_heads,
        preferred_element_type=jnp.float32,
    )
    sum_inside = jnp.sum(weight_inside, axis=-1)

    outside = jnp.where((segment == last_in)[None, :], cumulative + top_in[:, None], very_negative)
    peak_log = jnp.maximum(outside, peak_inside)
    carried = jnp.exp(outside - peak_log)
    local = jnp.exp(peak_inside - peak_log)
    readout = jnp.einsum(
        "hlk,hvk->hlv",
        query_heads.astype(jnp.float32),
        memory_in,
        precision=lax.Precision.HIGHEST,
    )
    numer = carried[:, :, None] * readout[:, :, :head_dim] + local[:, :, None] * from_block
    denom = carried * readout[:, :, head_dim] + local * sum_inside
    mixed = numer / jnp.maximum(jnp.abs(denom), jnp.exp(-peak_log))[:, :, None]
    mixed = jnp.transpose(mixed, (1, 0, 2)).reshape(tok_rows, -1).astype(jnp.bfloat16)

    own_rows = tok_rows // tp
    mixed_rows = mixed.reshape(tp, own_rows, -1)
    projected = 0.0
    for d in range(tp):
        piece = lax.dynamic_index_in_dim(mixed_rows, (me + d) % tp, 0, keepdims=False)
        if d:
            piece = turn(piece, "tp", d)
        projected = projected + jnp.dot(
            piece, w_out_parts[d], preferred_element_type=jnp.float32
        )
    middle = (residual.astype(jnp.float32) + projected).astype(jnp.bfloat16)
    middle_wide = middle.astype(jnp.float32)
    factor = lax.rsqrt(jnp.mean(middle_wide * middle_wide, axis=-1, keepdims=True) + epsilon)
    normed = (middle_wide * factor * norm_gain.astype(jnp.float32)).astype(jnp.bfloat16)

    gathered = normed
    for axis in ("tp", "x", "c"):
        gathered = jnp.concatenate(
            [gathered] + [turn(gathered, axis, d) for d in range(1, lax.axis_size(axis))], axis=0
        )
    lifted = jnp.dot(gathered, up_all, preferred_element_type=jnp.float32)
    hidden = jnp.square(jax.nn.relu(lifted)).astype(jnp.bfloat16)
    sizes = (lax.axis_size("c"), lax.axis_size("x"), tp)
    half = down_all.shape[1] // 2
    summed = []
    for k, order in enumerate((("c", "x", "tp"), ("c", "tp", "x"))):
        terms = jnp.dot(
            hidden, down_all[:, k * half : (k + 1) * half], preferred_element_type=jnp.float32
        )
        terms = terms.astype(jnp.bfloat16).reshape(*sizes, own_rows, half)
        names = ["c", "x", "tp"]
        for axis in order:
            terms = reduced(terms, names.index(axis), axis)
            names.remove(axis)
        summed.append(terms.astype(jnp.float32))
    return (middle_wide + jnp.concatenate(summed, axis=1)).astype(jnp.bfloat16)


MESH = pl.DeviceIdType.MESH
PAIR = 2
SUBS = 2
NT = (((1,), (1,)), ((), ()))
NN = (((1,), (0,)), ((), ()))


def dot(a, b, dims=NN):
    return lax.dot_general(a, b, dims, preferred_element_type=jnp.float32)


def thirds(value):
    high = value.astype(jnp.bfloat16)
    rest = value - high.astype(jnp.float32)
    middle = rest.astype(jnp.bfloat16)
    low = (rest - middle.astype(jnp.float32)).astype(jnp.bfloat16)
    return high, middle, low


def combine_rows(earlier, later):
    memory_one, normal_one, top_one, decay_one, first_one, last_one = earlier
    memory_two, normal_two, top_two, decay_two, first_two, last_two = later
    later_empty = first_two < 0.0
    earlier_empty = first_one < 0.0
    keep = later_empty | (first_two == last_two) & (first_two == last_one)
    decay_step = jnp.where(later_empty, 0.0, decay_two)
    top_new = jnp.where(keep, jnp.maximum(decay_step + top_one, top_two), top_two)
    scale_old = jnp.where(keep, jnp.exp(decay_step + top_one - top_new), 0.0)
    scale_new = jnp.exp(top_two - top_new)
    return (
        scale_old * memory_one + scale_new * memory_two,
        scale_old * normal_one + scale_new * normal_two,
        top_new,
        jnp.where(keep, decay_one + decay_step, decay_two),
        jnp.where(earlier_empty, first_two, first_one),
        jnp.where(later_empty, last_one, last_two),
    )


def choose(flag, one, two):
    return tuple(jnp.where(flag, a, b) for a, b in zip(one, two))


def layer_kernel(
    sizes,
    query_ref,
    key_ref,
    value_ref,
    in_ref,
    forget_ref,
    document_ref,
    gain_ref,
    residual_ref,
    w_out_ref,
    w_up_ref,
    w_down_ref,
    out_ref,
    up_buf,
    down_buf,
    wout_own,
    wout_far,
    residual_buf,
    states,
    totals,
    before,
    mixed_buf,
    mixed_far,
    gathered,
    hidden,
    middle_buf,
    part_send,
    part_far,
    weight_sem,
    z_sem,
    x_sem,
    d_sem,
    local_sem,
    state_sem,
    total_sem,
    mix_sem,
    gather_sem,
    part_sem,
    part_out_sem,
):
    nz, nx, nc, ny = sizes
    z, x, c, y = (lax.axis_index(name) for name in ("z", "x", "c", "tp"))
    zl = lax.rem(z, PAIR)
    zn = z + 1 - 2 * zl
    rows, width = query_ref.shape
    heads = in_ref.shape[0]
    pairs = heads // 2
    lanes = width // pairs
    hd = lanes // 2
    own = rows // ny
    model = out_ref.shape[1]
    depth = w_up_ref.shape[0]
    cols = w_down_ref.shape[1]
    units = w_up_ref.shape[1] // PAIR
    sub = units // SUBS
    plane = nx * nc
    spot = x * nc + c

    def remote(src, dst, send, recv, dev):
        return pltpu.make_async_remote_copy(
            src_ref=src,
            dst_ref=dst,
            send_sem=send,
            recv_sem=recv,
            device_id=dev,
            device_id_type=MESH,
        )

    x_dev = (z, 1 - x, c, y)
    c_dev = (z, x, 1 - c, y)
    y_dev = (z, x, c, 1 - y)

    def place(s, xx, cc):
        return (s * nx + xx) * nc + cc

    def slot(m, s, xx, cc, b):
        if m == 0:
            start = pl.multiple_of(place(s, xx, cc) * depth, depth)
            return up_buf.at[pl.ds(start, depth), pl.ds(b * sub, sub)]
        lane0 = pl.multiple_of(cc * cols, cols)
        return down_buf.at[s * nx + xx, pl.ds(b * sub, sub), pl.ds(lane0, cols)]

    def source(m, g, b):
        start = pl.multiple_of(g * units + b * sub, sub)
        if m == 0:
            return w_up_ref.at[:, pl.ds(start, sub)]
        return w_down_ref.at[pl.ds(start, sub), :]

    def send_z(m, k, g, s, to, b):
        src = source(m, g, b) if s is None else slot(m, s, x, c, b)
        s = z if s is None else s
        return remote(
            src,
            slot(m, s, x, c, b),
            z_sem.at[m, k, b],
            weight_sem.at[m, place(s, x, c), b],
            (jnp.int32(to), x, c, y),
        )

    def send_x(m, k, s, b):
        src = source(m, zl, b) if k == 0 else slot(m, s, x, c, b)
        return remote(
            src, slot(m, s, x, c, b), x_sem.at[m, k, b], weight_sem.at[m, place(s, x, c), b], x_dev
        )

    def send_c(m, k, s, far, b):
        xx = 1 - x if far else x
        src = source(m, zl, b) if k == 0 and not far else slot(m, s, xx, c, b)
        return remote(
            src,
            slot(m, s, xx, c, b),
            d_sem.at[m, k, int(far), b],
            weight_sem.at[m, place(s, xx, c), b],
            c_dev,
        )

    def arrived(m, s, xx, cc, b):
        remote(
            slot(m, s, xx, cc, b),
            slot(m, s, xx, cc, b),
            x_sem.at[m, 0, b],
            weight_sem.at[m, place(s, xx, cc), b],
            x_dev,
        ).wait_recv()

    def local(m, b):
        return pltpu.make_async_copy(source(m, zl, b), slot(m, z, x, c, b), local_sem.at[m, b])

    plan_left = {1: [(0, 0)], 2: [(0, 0), (1, 1)], 3: [(0, 2), (1, 1)]}
    plan_right = {0: [(1, 1), (0, 2)], 1: [(1, 3), (0, 2)], 2: [(1, 3)]}

    def on_line(m, part, act):
        for kz in range(nz):
            sends = [(g, to, False) for g, to in plan_left.get(kz, [])]
            sends += [(g, to, i > 0) for i, (g, to) in enumerate(plan_right.get(kz, []))]
            todo = [
                (k, g, to)
                for k, (g, to, late) in enumerate(sends)
                if part is None or part == late
            ]
            if not todo:
                continue

            @pl.when(z == kz)
            def _(todo=todo):
                for k, g, to in todo:
                    for b in range(SUBS):
                        act(send_z(m, k, g, None, to, b))

    def on_relay(m, bs, act):
        for kz, s, to in ((1, 0, 3), (2, 3, 0)):

            @pl.when(z == kz)
            def _(s=s, to=to):
                for b in bs:
                    act(send_z(m, 3, None, jnp.int32(s), to, b))

    start = lambda copy: copy.start()
    order = [z, zn, 2 - z // 2, (nz - 1) * (1 - z // 2)]

    barrier = pltpu.get_barrier_semaphore()
    partners = [(lax.rem(z + d, nz), x, c, y) for d in range(1, nz)]
    partners += [x_dev, c_dev, (z, 1 - x, 1 - c, y), y_dev, (zn, x, c, 1 - y)]
    for dev in partners:
        pl.semaphore_signal(barrier, inc=1, device_id=dev, device_id_type=MESH)

    load_residual = pltpu.make_async_copy(residual_ref, residual_buf, local_sem.at[2, 0])
    load_wout = pltpu.make_async_copy(w_out_ref, wout_own, local_sem.at[2, 1])
    load_residual.start()
    load_wout.start()
    for m in range(2):
        for b in range(SUBS):
            local(m, b).start()
    pl.semaphore_wait(barrier, len(partners))

    on_line(0, False, start)
    send_wout = remote(w_out_ref, wout_far, mix_sem.at[0], mix_sem.at[1], y_dev)
    send_wout.start()
    for b in range(SUBS):
        send_c(0, 0, z, False, b).start()
    send_x(0, 0, z, 0).start()

    near = lax.broadcasted_iota(jnp.int32, (1, lanes), 1) < hd
    forget = forget_ref[...]
    decay_log = jnp.minimum(forget, 0.0) - jnp.log1p(jnp.exp(-jnp.abs(forget)))
    gates = jnp.concatenate([decay_log, in_ref[...]], axis=0)
    at = lax.broadcasted_iota(jnp.int32, gates.shape, 1)
    running = gates
    step = 1
    while step < rows:
        running = running + jnp.where(at >= step, pltpu.roll(running, step, 1), 0.0)
        step *= 2
    cum_row = running[:heads]
    in_row = gates[heads:]
    seg_row = document_ref[...].astype(jnp.float32)
    seg_first = seg_row[:, 0:1]
    seg_last = seg_row[:, rows - 1 : rows]
    total = cum_row[:, rows - 1 : rows]
    growth = jnp.where(seg_row == seg_last, total - cum_row + in_row, very_negative)
    top = jnp.max(growth, axis=1, keepdims=True)
    summary = jnp.exp(growth - top)
    columns = jnp.transpose(jnp.concatenate([summary, cum_row], axis=0))
    seg_col = jnp.transpose(jnp.broadcast_to(seg_row, (2 * heads, rows)))[:, 0:1]

    row_of = lax.broadcasted_iota(jnp.int32, (8, lanes), 0)
    tall = hd + 8
    for p in range(pairs):
        a, b = 2 * p, 2 * p + 1
        span = pl.ds(p * lanes, lanes)
        keys = key_ref[:, span].astype(jnp.float32)
        weighted = keys * jnp.where(near, columns[:, a : a + 1], columns[:, b : b + 1])
        values_t = jnp.transpose(value_ref[:, span])
        full = sum(dot(values_t, piece) for piece in thirds(weighted))
        memory = jnp.where(near, full[:hd], full[hd:])
        normal = jnp.sum(weighted, axis=0, keepdims=True)
        top_row = jnp.where(near, top[a : a + 1], top[b : b + 1])
        decay_row = jnp.where(near, total[a : a + 1], total[b : b + 1])
        info = jnp.where(row_of == 0, normal, 0.0)
        for i, line in enumerate((top_row, decay_row, seg_first, seg_last)):
            info = jnp.where(row_of == i + 1, line, info)
        states[spot, p * tall : p * tall + hd, :] = memory
        states[spot, p * tall + hd : (p + 1) * tall, :] = info

    def send_state(k, dx, dc):
        dev = (z, lax.rem(x + dx, nx), lax.rem(c + dc, nc), y)
        return remote(
            states.at[spot], states.at[spot], state_sem.at[0, k], state_sem.at[1, spot], dev
        )

    state_sends = [send_state(k, k // nc, k % nc) for k in range(1, plane)]
    for copy in state_sends:
        copy.start()
    for b in range(1, SUBS):
        send_x(0, 0, z, b).start()

    row_ids = lax.broadcasted_iota(jnp.int32, (rows, rows), 0)
    col_ids = lax.broadcasted_iota(jnp.int32, (rows, rows), 1)
    allowed = (col_ids <= row_ids) & (seg_col == seg_row)
    inner = []
    for p in range(pairs):
        span = pl.ds(p * lanes, lanes)
        queries = query_ref[:, span] * jnp.asarray(hd**-0.5, jnp.bfloat16)
        keys = key_ref[:, span]
        values = value_ref[:, span]
        zero = jnp.zeros_like(queries)
        peaks, sums, outs = [], [], []
        for i in range(2):
            h = 2 * p + i
            mine = near if i == 0 else jnp.logical_not(near)
            scores = dot(jnp.where(mine, queries, zero), keys, NT)
            cum_col = columns[:, heads + h : heads + h + 1]
            inside = jnp.where(
                allowed, cum_col - cum_row[h : h + 1] + in_row[h : h + 1], very_negative
            )
            peak = jnp.max(inside, axis=1, keepdims=True)
            weight = jnp.exp(inside - peak) * scores
            peaks.append(peak)
            sums.append(jnp.sum(weight, axis=1, keepdims=True))
            outs.append(dot(weight.astype(jnp.bfloat16), jnp.where(mine, values, zero)))
        cum_pair = jnp.where(
            near,
            columns[:, heads + 2 * p : heads + 2 * p + 1],
            columns[:, heads + 2 * p + 1 : heads + 2 * p + 2],
        )
        inner.append(
            (
                queries,
                cum_pair,
                jnp.where(near, peaks[0], peaks[1]),
                jnp.where(near, sums[0], sums[1]),
                outs[0] + outs[1],
            )
        )

    def load(ref, i, p):
        info = ref[i, p * tall + hd : (p + 1) * tall, :]
        return (ref[i, p * tall : p * tall + hd, :],) + tuple(info[j : j + 1] for j in range(5))

    def empty():
        zero = jnp.zeros((1, lanes), jnp.float32)
        return (
            jnp.zeros((hd, lanes), jnp.float32),
            zero,
            zero + very_negative,
            zero,
            zero - 1.0,
            zero - 1.0,
        )

    def store(ref, i, p, state):
        info = jnp.zeros((8, lanes), jnp.float32)
        for j, line in enumerate(state[1:]):
            info = jnp.where(row_of == j, line, info)
        ref[i, p * tall : p * tall + hd, :] = state[0]
        ref[i, p * tall + hd : (p + 1) * tall, :] = info

    for dx in range(nx):
        for dc in range(nc):
            if dx or dc:
                other = lax.rem(x + dx, nx) * nc + lax.rem(c + dc, nc)
                remote(
                    states.at[other],
                    states.at[other],
                    state_sem.at[0, dx * nc + dc],
                    state_sem.at[1, other],
                    c_dev,
                ).wait_recv()
    prefix = []
    for p in range(pairs):
        running_state = load(states, 0, p)
        mine = choose(spot == 0, empty(), running_state)
        for i in range(1, plane):
            if i > 1:
                mine = choose(spot == i, running_state, mine)
            later = load(states, i, p)
            if i == 1:
                mine = choose(spot >= 1, running_state, mine)
            running_state = combine_rows(running_state, later)
        prefix.append(mine)
        store(totals, 0, p, running_state)

    back = before.shape[0]

    def send_total(d):
        return remote(
            totals.at[0],
            before.at[d - 1],
            total_sem.at[0, d - 1],
            total_sem.at[1, d - 1],
            (lax.rem(z + d, nz), x, c, y),
        )

    for d in range(1, back + 1):
        pl.when(z + d < nz)(lambda d=d: send_total(d).start())
    on_line(0, True, start)

    for d in range(1, back + 1):
        pl.when(z >= d)(lambda d=d: send_total(d).wait_recv())

        @pl.when(z < d)
        def _(d=d):
            for p in range(pairs):
                store(before, d - 1, p, empty())

    wide_near = lax.broadcasted_iota(jnp.int32, (lanes, lanes), 1) < hd
    wide_top = lax.broadcasted_iota(jnp.int32, (lanes, lanes), 0) < hd
    block = wide_near == wide_top
    for p in range(pairs):
        queries, cum_pair, peak_in, sum_in, from_block = inner[p]
        incoming = load(before, back - 1, p)
        for d in range(back - 1, 0, -1):
            incoming = combine_rows(incoming, load(before, d - 1, p))
        memory, normal, top_row, _, _, last_row = combine_rows(incoming, prefix[p])
        outside = jnp.where(seg_col == last_row, cum_pair + top_row, very_negative)
        peak = jnp.maximum(outside, peak_in)
        carried = jnp.exp(outside - peak)
        inside = jnp.exp(peak_in - peak)
        keep = jnp.where(block, jnp.concatenate([memory, memory], axis=0), 0.0)
        norms = jnp.where(block, jnp.broadcast_to(normal, (lanes, lanes)), 0.0)
        both = jnp.concatenate([keep, norms], axis=0)
        readout = sum(dot(queries, piece, NT) for piece in thirds(both))
        numer = carried * readout[:, :lanes] + inside * from_block
        denom = carried * readout[:, lanes:] + inside * sum_in
        mixed = numer / jnp.maximum(jnp.abs(denom), jnp.exp(-peak))
        mixed_buf[:, p * lanes : (p + 1) * lanes] = mixed.astype(jnp.bfloat16)

    far_rows = pl.ds(pl.multiple_of((1 - y) * own, own), own)
    own_rows = pl.ds(pl.multiple_of(y * own, own), own)
    send_mixed = remote(mixed_buf.at[far_rows], mixed_far, mix_sem.at[2], mix_sem.at[3], y_dev)
    send_mixed.start()

    def relay_near(m, k, s):
        for b in range(SUBS):
            arrived(m, s, x, c, b)
            if k == 1:
                on_relay(m, (b,), start)
            send_x(m, k, s, b).start()
            send_c(m, k, s, False, b).start()

    def relay_far(m, k, s):
        for b in range(SUBS):
            arrived(m, s, 1 - x, c, b)
            send_c(m, k, s, True, b).start()

    load_residual.wait()
    load_wout.wait()
    projected = dot(mixed_buf[own_rows, :], wout_own[...])
    send_wout.wait_recv()
    send_mixed.wait_recv()
    projected = projected + dot(mixed_far[...], wout_far[...])
    middle = (residual_buf[...].astype(jnp.float32) + projected).astype(jnp.bfloat16)
    middle_buf[...] = middle
    wide = middle.astype(jnp.float32)
    factor = lax.rsqrt(jnp.mean(wide * wide, axis=-1, keepdims=True) + epsilon)
    me = zl * ny + y
    my_rows = pl.ds(pl.multiple_of(me * own, own), own)
    gathered[my_rows, :] = (wide * factor * gain_ref[...].astype(jnp.float32)).astype(jnp.bfloat16)
    group = [(z, 1 - y, zl), (zn, y, 1 - zl), (zn, 1 - y, 1 - zl)]
    gather_sends = [
        remote(
            gathered.at[my_rows],
            gathered.at[my_rows],
            gather_sem.at[0, r],
            gather_sem.at[1, me],
            (pz, x, c, py),
        )
        for r, (pz, py, _) in enumerate(group)
    ]
    for copy in gather_sends:
        copy.start()

    relay_near(0, 1, order[1])
    on_line(1, None, start)
    for b in range(SUBS):
        send_c(1, 0, z, False, b).start()
    relay_far(0, 0, order[0])
    relay_near(0, 2, order[2])
    relay_far(0, 1, order[1])
    relay_near(0, 3, order[3])
    for b in range(SUBS):
        send_x(1, 0, z, b).start()
    relay_far(0, 2, order[2])
    relay_far(0, 3, order[3])
    for m in range(2):
        for b in range(SUBS):
            local(m, b).wait()
    for s in order:
        for xx in range(nx):
            for b in range(SUBS):
                arrived(0, s, lax.rem(x + xx, nx), 1 - c, b)
    for _, py, pl_z in group:
        other = pl_z * ny + py
        there = pl.ds(pl.multiple_of(other * own, own), own)
        remote(
            gathered.at[there],
            gathered.at[there],
            gather_sem.at[0, 0],
            gather_sem.at[1, other],
            y_dev,
        ).wait_recv()

    tile = nc * cols

    def lift(i, carry):
        at_units = pl.ds(pl.multiple_of(i * tile, tile), tile)
        lifted = dot(gathered[...], up_buf[:, at_units])
        positive = jnp.maximum(lifted, 0.0)
        hidden[:, at_units] = (positive * positive).astype(jnp.bfloat16)
        return carry

    lax.fori_loop(0, units // tile, lift, 0)

    def send_part(j, r):
        pz, py, pzl = group[r]
        other = pzl * ny + py
        return remote(
            part_send.at[j, other],
            part_far.at[j, me],
            part_out_sem.at[j, r],
            part_sem.at[j, me],
            (pz, x, c, py),
        )

    def lower(s, xx):
        j = s * nx + xx
        for b in range(SUBS):
            arrived(1, s, xx, 1 - c, b)
        terms = dot(hidden[...], down_buf[j])
        rounded = terms.astype(jnp.bfloat16)
        for t in range(PAIR * ny):
            part_send[j, t] = rounded[t * own : (t + 1) * own]
        for r in range(len(group)):
            send_part(j, r).start()

    def finish(s, xx):
        j = s * nx + xx
        summed = part_send[j, me].astype(jnp.float32)
        for _, py, pzl in group:
            other = pzl * ny + py
            remote(
                part_send.at[j, other],
                part_far.at[j, other],
                part_out_sem.at[j, 0],
                part_sem.at[j, other],
                y_dev,
            ).wait_recv()
            summed = summed + part_far[j, other].astype(jnp.float32)
        at_cols = pl.ds(pl.multiple_of(j * tile, tile), tile)
        out_ref[:, at_cols] = (middle_buf[:, at_cols].astype(jnp.float32) + summed).astype(
            jnp.bfloat16
        )

    for k in range(nz):
        s = order[k]
        if k + 1 < nz:
            relay_near(1, k + 1, order[k + 1])
        relay_far(1, k, s)

        def both(i, carry, s=s):
            lower(s, lax.rem(x + i, nx))
            return carry

        lax.fori_loop(0, nx, both, 0)
        if k:

            def ends(i, carry, s=order[k - 1]):
                finish(s, lax.rem(x + i, nx))
                return carry

            lax.fori_loop(0, nx, ends, 0)
    for i in range(nx):
        finish(order[nz - 1], lax.rem(x + i, nx))

    wait = lambda copy: copy.wait_send()
    for m in range(2):
        on_line(m, None, wait)
        on_relay(m, range(SUBS), wait)
        for k in range(nz):
            for b in range(SUBS):
                wait(send_x(m, k, order[k], b))
                wait(send_c(m, k, order[k], False, b))
                wait(send_c(m, k, order[k], True, b))
    for copy in state_sends + gather_sends + [send_wout, send_mixed]:
        wait(copy)
    for d in range(1, back + 1):
        pl.when(z + d < nz)(lambda d=d: send_total(d).wait_send())

    def drained(j, carry):
        for r in range(len(group)):
            wait(send_part(j, r))
        return carry

    lax.fori_loop(0, nz * nx, drained, 0)


def fused(
    residual,
    query_vectors,
    key_vectors,
    value_vectors,
    in_gate,
    forget_gate,
    documents,
    w_out,
    norm_gain,
    w_up,
    w_down,
):
    sizes = tuple(lax.axis_size(name) for name in ("z", "x", "c", "tp"))
    nz, nx, nc, ny = sizes
    rows, width = query_vectors.shape
    heads = in_gate.shape[0]
    own, model = residual.shape
    depth, cols = w_up.shape[0], w_down.shape[1]
    units = w_up.shape[1] // PAIR
    members = PAIR * ny
    plane = nx * nc
    pairs = heads // 2
    state = (pairs * (width // heads + 8), width // pairs)
    reach = min(nz * plane - 1, -(-(DOC_MOST - 1) // rows))
    back = -(-reach // plane)
    bf16, f32 = jnp.bfloat16, jnp.float32
    dma = pltpu.SemaphoreType.DMA
    vmem = pl.BlockSpec(memory_space=pltpu.VMEM)
    anywhere = pl.BlockSpec(memory_space=pl.ANY)
    return pl.pallas_call(
        functools.partial(layer_kernel, sizes),
        out_shape=jax.ShapeDtypeStruct((own, model), bf16),
        in_specs=[vmem] * 7 + [anywhere] * 4,
        out_specs=vmem,
        scratch_shapes=[
            pltpu.VMEM((nz * plane * depth, units), bf16),
            pltpu.VMEM((nz * nx, units, nc * cols), bf16),
            pltpu.VMEM(w_out.shape, bf16),
            pltpu.VMEM(w_out.shape, bf16),
            pltpu.VMEM((own, model), bf16),
            pltpu.VMEM((plane,) + state, f32),
            pltpu.VMEM((1,) + state, f32),
            pltpu.VMEM((back,) + state, f32),
            pltpu.VMEM((rows, width), bf16),
            pltpu.VMEM((own, width), bf16),
            pltpu.VMEM((members * own, model), bf16),
            pltpu.VMEM((members * own, units), bf16),
            pltpu.VMEM((own, model), bf16),
            pltpu.VMEM((nz * nx, members, own, nc * cols), bf16),
            pltpu.VMEM((nz * nx, members, own, nc * cols), bf16),
            dma((2, nz * plane, SUBS)),
            dma((2, 4, SUBS)),
            dma((2, nz, SUBS)),
            dma((2, nz, 2, SUBS)),
            dma((3, 2)),
            dma((2, plane)),
            dma((2, back)),
            dma((4,)),
            dma((2, members)),
            dma((nz * nx, members)),
            dma((nz * nx, members - 1)),
        ],
        compiler_params=pltpu.CompilerParams(
            collective_id=0, has_side_effects=True, vmem_limit_bytes=60 * 1024 * 1024
        ),
    )(
        query_vectors,
        key_vectors,
        value_vectors,
        in_gate,
        forget_gate,
        documents.reshape(1, rows),
        norm_gain.reshape(1, model),
        residual,
        w_out,
        w_up,
        w_down,
    )


def suits(shape, args):
    nz, nx, nc, ny = shape
    query_vectors, in_gate, w_up, w_down = args[1], args[4], args[9], args[10]
    total, width = query_vectors.shape
    depth, cols = w_up.shape[0] // (nz * nx * nc), w_down.shape[1] // (nz * nx * nc)
    heads = in_gate.shape[0] // ny
    return (
        (nz, nx, nc, ny) == (2 * PAIR, 2, 2, 2)
        and depth % 128 == 0
        and cols % 128 == 0
        and heads == 4
        and width // in_gate.shape[0] == 64
        and total // (nz * nx * nc) == 256
    )


def solution(mesh):
    sp, tp = mesh.shape["sp"], mesh.shape["tp"]
    chips = tp if sp % (2 * tp) == 0 else 1
    cores = 2 if sp % 2 == 0 else 1
    shape = (sp // (chips * cores), chips, cores, tp)
    split = Mesh(np.asarray(mesh.devices).reshape(shape), ("z", "x", "c", "tp"))
    placed = (
        P(("z", "x", "c", "tp"), None),
        P(SP, "tp"),
        P(SP, "tp"),
        P(SP, "tp"),
        P("tp", SP),
        P("tp", SP),
        P(SP),
        P("tp", None),
        P(),
        P(SP, "tp"),
        P("tp", SP),
    )

    def run(*args):
        return jax.shard_map(
            fused if suits(shape, args) else on_device,
            mesh=split,
            in_specs=placed,
            out_specs=P(("z", "x", "c", "tp"), None),
            check_vma=False,
        )(*args)

    return run
```

```python
import functools

import jax
import jax.numpy as jnp
import numpy as np
from jax import lax
from jax.experimental import pallas as pl
from jax.experimental.pallas import tpu as pltpu
from jax.sharding import Mesh, PartitionSpec as P

DOC_MOST = 2048
very_negative = -1e30
epsilon = 1e-06
SP = ("z", "x", "c")
G = ("x", "c")


def combine(earlier, later):
    memory_one, top_one, decay_one, first_one, last_one = earlier
    memory_two, top_two, decay_two, first_two, last_two = later
    later_empty = first_two < 0.0
    earlier_empty = first_one < 0.0
    keep = later_empty | (first_two == last_two) & (first_two == last_one)
    decay_step = jnp.where(later_empty, 0.0, decay_two)
    top_new = jnp.where(keep, jnp.maximum(decay_step + top_one, top_two), top_two)
    scale_old = jnp.where(keep, jnp.exp(decay_step + top_one - top_new), 0.0)
    scale_new = jnp.exp(top_two - top_new)
    memory_new = scale_old[:, None, None] * memory_one + scale_new[:, None, None] * memory_two
    decay_new = jnp.where(keep, decay_one + decay_step, decay_two)
    first_new = jnp.where(earlier_empty, first_two, first_one)
    last_new = jnp.where(later_empty, last_one, last_two)
    return (memory_new, top_new, decay_new, first_new, last_new)


def pack(state):
    memory, top, decay, first, last = state
    heads, _, width = memory.shape
    row = jnp.stack(
        [top, decay, jnp.broadcast_to(first, top.shape), jnp.broadcast_to(last, top.shape)], axis=1
    )
    row = jnp.pad(row, ((0, 0), (0, width - 4)))
    return jnp.concatenate(
        [memory, row[:, None, :], jnp.zeros((heads, 6, width), jnp.float32)], axis=1
    )


def unpack(packed, present):
    rows = packed.shape[1] - 7
    row = packed[:, rows]
    memory = jnp.where(present, packed[:, :rows], 0.0)
    top = jnp.where(present, row[:, 0], very_negative)
    decay = jnp.where(present, row[:, 1], 0.0)
    first = jnp.where(present, row[0, 2], -1.0)
    last = jnp.where(present, row[0, 3], -1.0)
    return (memory, top, decay, first, last)


def shifted(state, distance, length, here):
    packed = lax.ppermute(pack(state), SP, [(i, i + distance) for i in range(length - distance)])
    return unpack(packed, here >= distance)


def turn(value, axis, d):
    n = lax.axis_size(axis)
    return lax.ppermute(value, axis, [(i, (i + d) % n) for i in range(n)])


def reduced(terms, dim, axis):
    def block(d):
        return lax.index_in_dim(terms, d, dim, keepdims=False)

    total = block(0).astype(jnp.float32)
    for d in range(1, lax.axis_size(axis)):
        total = total + turn(block(d), axis, -d).astype(jnp.float32)
    return total.astype(jnp.bfloat16)


def on_device(
    residual,
    query_vectors,
    key_vectors,
    value_vectors,
    in_gate,
    forget_gate,
    documents,
    w_out,
    norm_gain,
    w_up,
    w_down,
):
    tok_rows = query_vectors.shape[0]
    heads = in_gate.shape[0]
    head_dim = query_vectors.shape[1] // heads
    length = lax.axis_size(SP)
    here = lax.axis_index(SP)
    tp = lax.axis_size("tp")
    me = lax.axis_index("tp")

    plane = lax.axis_size(G)
    up_pieces = jnp.transpose(w_up.reshape(w_up.shape[0], plane, -1), (1, 0, 2))
    up_part = lax.all_to_all(up_pieces, G, split_axis=0, concat_axis=0, tiled=True)
    up_part = up_part.reshape(-1, up_part.shape[-1])
    up_part, w_down, w_out, key_vectors, in_gate, forget_gate, documents = (
        lax.optimization_barrier(
            (up_part, w_down, w_out, key_vectors, in_gate, forget_gate, documents)
        )
    )
    down_part = lax.all_to_all(w_down, G, split_axis=0, concat_axis=1, tiled=True)
    up_all = lax.all_gather(up_part, "z", axis=0, tiled=True)
    down_all = lax.all_gather(down_part, "z", axis=1, tiled=True)

    w_out_parts = [w_out] + [turn(w_out, "tp", d) for d in range(1, tp)]

    segment = documents.astype(jnp.float32)
    decay_log = jax.nn.log_sigmoid(forget_gate)
    cumulative = jnp.cumsum(decay_log, axis=-1)
    key_heads = jnp.transpose(key_vectors.reshape(tok_rows, heads, head_dim), (1, 0, 2))
    value_heads = jnp.transpose(value_vectors.reshape(tok_rows, heads, head_dim), (1, 0, 2))
    query_heads = jnp.transpose(query_vectors.reshape(tok_rows, heads, head_dim), (1, 0, 2))
    query_heads = query_heads * jnp.asarray(head_dim ** (-0.5), query_heads.dtype)
    latest = segment == segment[-1]
    growth = jnp.where(latest[None, :], cumulative[:, -1:] - cumulative + in_gate, very_negative)
    top_log = jnp.max(growth, axis=-1)
    summary_weight = jnp.exp(growth - top_log[:, None])
    key_wide = key_heads.astype(jnp.float32)
    weighted = key_wide * summary_weight[:, :, None]
    memory = jnp.einsum(
        "hsv,hsk->hvk", value_heads.astype(jnp.float32), weighted, precision=lax.Precision.HIGHEST
    )
    normal = jnp.sum(weighted, axis=1)
    state = (
        jnp.concatenate([memory, normal[:, None, :]], axis=1),
        top_log,
        cumulative[:, -1],
        segment[0],
        segment[-1],
    )

    reach = min(length - 1, -(-(DOC_MOST - 1) // tok_rows))
    span = 1
    while span < reach:
        state = combine(shifted(state, span, length, here), state)
        span *= 2
    incoming = shifted(state, 1, length, here)
    memory_in, top_in, _, _, last_in = incoming

    row_ids = lax.broadcasted_iota(jnp.int32, (tok_rows, tok_rows), 0)
    col_ids = lax.broadcasted_iota(jnp.int32, (tok_rows, tok_rows), 1)
    allowed = (col_ids <= row_ids) & (segment[:, None] == segment[None, :])
    inside = jnp.where(
        allowed[None],
        cumulative[:, :, None] - cumulative[:, None, :] + in_gate[:, None, :],
        very_negative,
    )
    peak_inside = jnp.max(inside, axis=-1)
    scores = jnp.einsum(
        "hld,hsd->hls", query_heads, key_heads, preferred_element_type=jnp.float32
    )
    weight_inside = jnp.exp(inside - peak_inside[:, :, None]) * scores
    from_block = jnp.einsum(
        "hls,hsv->hlv",
        weight_inside.astype(jnp.bfloat16),
        value_heads,
        preferred_element_type=jnp.float32,
    )
    sum_inside = jnp.sum(weight_inside, axis=-1)

    outside = jnp.where((segment == last_in)[None, :], cumulative + top_in[:, None], very_negative)
    peak_log = jnp.maximum(outside, peak_inside)
    carried = jnp.exp(outside - peak_log)
    local = jnp.exp(peak_inside - peak_log)
    readout = jnp.einsum(
        "hlk,hvk->hlv",
        query_heads.astype(jnp.float32),
        memory_in,
        precision=lax.Precision.HIGHEST,
    )
    numer = carried[:, :, None] * readout[:, :, :head_dim] + local[:, :, None] * from_block
    denom = carried * readout[:, :, head_dim] + local * sum_inside
    mixed = numer / jnp.maximum(jnp.abs(denom), jnp.exp(-peak_log))[:, :, None]
    mixed = jnp.transpose(mixed, (1, 0, 2)).reshape(tok_rows, -1).astype(jnp.bfloat16)

    own_rows = tok_rows // tp
    mixed_rows = mixed.reshape(tp, own_rows, -1)
    projected = 0.0
    for d in range(tp):
        piece = lax.dynamic_index_in_dim(mixed_rows, (me + d) % tp, 0, keepdims=False)
        if d:
            piece = turn(piece, "tp", d)
        projected = projected + jnp.dot(
            piece, w_out_parts[d], preferred_element_type=jnp.float32
        )
    middle = (residual.astype(jnp.float32) + projected).astype(jnp.bfloat16)
    middle_wide = middle.astype(jnp.float32)
    factor = lax.rsqrt(jnp.mean(middle_wide * middle_wide, axis=-1, keepdims=True) + epsilon)
    normed = (middle_wide * factor * norm_gain.astype(jnp.float32)).astype(jnp.bfloat16)

    gathered = normed
    for axis in ("tp", "x", "c"):
        gathered = jnp.concatenate(
            [gathered] + [turn(gathered, axis, d) for d in range(1, lax.axis_size(axis))], axis=0
        )
    lifted = jnp.dot(gathered, up_all, preferred_element_type=jnp.float32)
    hidden = jnp.square(jax.nn.relu(lifted)).astype(jnp.bfloat16)
    sizes = (lax.axis_size("c"), lax.axis_size("x"), tp)
    half = down_all.shape[1] // 2
    summed = []
    for k, order in enumerate((("c", "x", "tp"), ("c", "tp", "x"))):
        terms = jnp.dot(
            hidden, down_all[:, k * half : (k + 1) * half], preferred_element_type=jnp.float32
        )
        terms = terms.astype(jnp.bfloat16).reshape(*sizes, own_rows, half)
        names = ["c", "x", "tp"]
        for axis in order:
            terms = reduced(terms, names.index(axis), axis)
            names.remove(axis)
        summed.append(terms.astype(jnp.float32))
    return (middle_wide + jnp.concatenate(summed, axis=1)).astype(jnp.bfloat16)


MESH = pl.DeviceIdType.MESH
PAIR = 2
SUBS = 4
NT = (((1,), (1,)), ((), ()))
NN = (((1,), (0,)), ((), ()))


def dot(a, b, dims=NN):
    return lax.dot_general(a, b, dims, preferred_element_type=jnp.float32)


def thirds(value):
    high = value.astype(jnp.bfloat16)
    rest = value - high.astype(jnp.float32)
    middle = rest.astype(jnp.bfloat16)
    low = (rest - middle.astype(jnp.float32)).astype(jnp.bfloat16)
    return high, middle, low


def combine_rows(earlier, later):
    memory_one, normal_one, top_one, decay_one, first_one, last_one = earlier
    memory_two, normal_two, top_two, decay_two, first_two, last_two = later
    later_empty = first_two < 0.0
    earlier_empty = first_one < 0.0
    keep = later_empty | (first_two == last_two) & (first_two == last_one)
    decay_step = jnp.where(later_empty, 0.0, decay_two)
    top_new = jnp.where(keep, jnp.maximum(decay_step + top_one, top_two), top_two)
    scale_old = jnp.where(keep, jnp.exp(decay_step + top_one - top_new), 0.0)
    scale_new = jnp.exp(top_two - top_new)
    return (
        scale_old * memory_one + scale_new * memory_two,
        scale_old * normal_one + scale_new * normal_two,
        top_new,
        jnp.where(keep, decay_one + decay_step, decay_two),
        jnp.where(earlier_empty, first_two, first_one),
        jnp.where(later_empty, last_one, last_two),
    )


def choose(flag, one, two):
    return tuple(jnp.where(flag, a, b) for a, b in zip(one, two))


def layer_kernel(
    sizes,
    query_ref,
    key_ref,
    value_ref,
    in_ref,
    forget_ref,
    document_ref,
    gain_ref,
    residual_ref,
    w_out_ref,
    w_up_ref,
    w_down_ref,
    out_ref,
    up_buf,
    down_buf,
    wout_own,
    wout_far,
    residual_buf,
    states,
    totals,
    before,
    mixed_buf,
    mixed_far,
    gathered,
    hidden,
    middle_buf,
    part_own,
    part_y,
    part_y_far,
    part_z,
    part_z_far,
    out_buf,
    weight_sem,
    z_sem,
    x_sem,
    d_sem,
    local_sem,
    state_sem,
    total_sem,
    mix_sem,
    wout_sem,
    gather_sem,
    part_y_sem,
    part_z_sem,
    out_sem,
):
    nz, nx, nc, ny = sizes
    z, x, c, y = (lax.axis_index(name) for name in ("z", "x", "c", "tp"))
    zl = z // PAIR
    zn = lax.rem(z + PAIR, nz)
    rows, width = query_ref.shape
    heads = in_ref.shape[0]
    pairs = heads // 2
    lanes = width // pairs
    hd = lanes // 2
    own = rows // ny
    model = out_ref.shape[1]
    depth = w_up_ref.shape[0]
    cols = w_down_ref.shape[1]
    units = w_up_ref.shape[1] // PAIR
    sub = units // SUBS
    plane = nx * nc
    spot = x * nc + c
    tile = nc * cols

    def remote(src, dst, send, recv, dev):
        return pltpu.make_async_remote_copy(
            src_ref=src,
            dst_ref=dst,
            send_sem=send,
            recv_sem=recv,
            device_id=dev,
            device_id_type=MESH,
        )

    x_dev = (z, 1 - x, c, y)
    c_dev = (z, x, 1 - c, y)
    y_dev = (z, x, c, 1 - y)
    n_dev = (zn, x, c, y)

    def place(s, xx, cc):
        return (s * nx + xx) * nc + cc

    def slot(m, s, xx, cc, b):
        if m == 0:
            start = pl.multiple_of(place(s, xx, cc) * depth, depth)
            return up_buf.at[pl.ds(start, depth), pl.ds(b * sub, sub)]
        lane0 = pl.multiple_of(cc * cols, cols)
        return down_buf.at[s * nx + xx, pl.ds(b * sub, sub), pl.ds(lane0, cols)]

    def source(m, g, b):
        start = pl.multiple_of(g * units + b * sub, sub)
        if m == 0:
            return w_up_ref.at[:, pl.ds(start, sub)]
        return w_down_ref.at[pl.ds(start, sub), :]

    def send_z(m, k, g, s, to, b):
        src = source(m, g, b) if s is None else slot(m, s, x, c, b)
        s = z if s is None else s
        return remote(
            src,
            slot(m, s, x, c, b),
            z_sem.at[m, k, b],
            weight_sem.at[m, place(s, x, c), b],
            (jnp.int32(to), x, c, y),
        )

    def send_x(m, k, s, b):
        src = source(m, zl, b) if k == 0 else slot(m, s, x, c, b)
        return remote(
            src, slot(m, s, x, c, b), x_sem.at[m, k, b], weight_sem.at[m, place(s, x, c), b], x_dev
        )

    def send_c(m, k, s, far, b):
        xx = 1 - x if far else x
        src = source(m, zl, b) if k == 0 and not far else slot(m, s, xx, c, b)
        return remote(
            src,
            slot(m, s, xx, c, b),
            d_sem.at[m, k, int(far), b],
            weight_sem.at[m, place(s, xx, c), b],
            c_dev,
        )

    def arrived(m, s, xx, cc, b):
        remote(
            slot(m, s, xx, cc, b),
            slot(m, s, xx, cc, b),
            x_sem.at[m, 0, b],
            weight_sem.at[m, place(s, xx, cc), b],
            x_dev,
        ).wait_recv()

    def local(m, b):
        return pltpu.make_async_copy(source(m, zl, b), slot(m, z, x, c, b), local_sem.at[m, b])

    to_left = {1: [(0, 0)], 2: [(0, 1)], 3: [(1, 2), (0, 1)]}
    to_right = {0: [(0, 1), (1, 2)], 1: [(1, 2)], 2: [(1, 3)]}

    def on_line(m, places, act, late=(False, True)):
        for kz in places:
            lefts, rights = to_left.get(kz, []), to_right.get(kz, [])
            todo = []
            for i, (g, to) in enumerate(lefts + rights):
                for b in range(SUBS):
                    behind = i > len(lefts) or (i == len(lefts) and b >= ahead[kz])
                    if behind in late:
                        todo.append((i, g, to, b))

            @pl.when(z == kz)
            def _(todo=todo):
                for i, g, to, b in todo:
                    act(send_z(m, i, g, None, to, b))

    ends, mids = (0, nz - 1), tuple(range(1, nz - 1))
    ahead = (1, 2, 2, 0)
    inside_line = (z > 0) & (z < nz - 1)

    def on_relay(m, k, b, act):
        for kz, to in ((1, 0), (2, 3)):
            pl.when(z == kz)(lambda to=to: act(send_z(m, k, None, order[k], to, b)))

    start = lambda copy: copy.start()
    order = [z, z + 1 - 2 * lax.rem(z, PAIR), 2 - z // 2, (nz - 1) * (1 - z // 2)]

    barrier = pltpu.get_barrier_semaphore()
    partners = [(lax.rem(z + d, nz), x, c, y) for d in range(1, nz)]
    partners += [x_dev, c_dev, (z, 1 - x, 1 - c, y), y_dev]
    for dev in partners:
        pl.semaphore_signal(barrier, inc=1, device_id=dev, device_id_type=MESH)

    load_residual = pltpu.make_async_copy(residual_ref, residual_buf, local_sem.at[2, 0])
    load_wout = pltpu.make_async_copy(w_out_ref, wout_own, local_sem.at[2, 1])
    load_residual.start()
    load_wout.start()
    for m in range(2):
        for b in range(SUBS):
            local(m, b).start()

    near = lax.broadcasted_iota(jnp.int32, (1, lanes), 1) < hd
    forget = forget_ref[...]
    decay_log = jnp.minimum(forget, 0.0) - jnp.log1p(jnp.exp(-jnp.abs(forget)))
    gates = jnp.concatenate([decay_log, in_ref[...]], axis=0)
    at = lax.broadcasted_iota(jnp.int32, gates.shape, 1)
    running = gates
    step = 1
    while step < rows:
        running = running + jnp.where(at >= step, pltpu.roll(running, step, 1), 0.0)
        step *= 2
    cum_row = running[:heads]
    in_row = gates[heads:]
    seg_row = document_ref[...].astype(jnp.float32)
    seg_first = seg_row[:, 0:1]
    seg_last = seg_row[:, rows - 1 : rows]
    total = cum_row[:, rows - 1 : rows]
    growth = jnp.where(seg_row == seg_last, total - cum_row + in_row, very_negative)
    top = jnp.max(growth, axis=1, keepdims=True)
    summary = jnp.exp(growth - top)
    columns = jnp.transpose(jnp.concatenate([summary, cum_row], axis=0))
    seg_col = jnp.transpose(jnp.broadcast_to(seg_row, (2 * heads, rows)))[:, 0:1]

    row_of = lax.broadcasted_iota(jnp.int32, (8, lanes), 0)
    tall = hd + 8

    def store(ref, i, p, state):
        info = jnp.zeros((8, lanes), jnp.float32)
        for j, line in enumerate(state[1:]):
            info = jnp.where(row_of == j, line, info)
        ref[i, p * tall : p * tall + hd, :] = state[0]
        ref[i, p * tall + hd : (p + 1) * tall, :] = info

    for p in range(pairs):
        a, b = 2 * p, 2 * p + 1
        span = pl.ds(p * lanes, lanes)
        keys = key_ref[:, span].astype(jnp.float32)
        weighted = keys * jnp.where(near, columns[:, a : a + 1], columns[:, b : b + 1])
        values_t = jnp.transpose(value_ref[:, span])
        full = sum(dot(values_t, piece) for piece in thirds(weighted))
        memory = jnp.where(near, full[:hd], full[hd:])
        normal = jnp.sum(weighted, axis=0, keepdims=True)
        top_row = jnp.where(near, top[a : a + 1], top[b : b + 1])
        decay_row = jnp.where(near, total[a : a + 1], total[b : b + 1])
        store(states, spot, p, (memory, normal, top_row, decay_row, seg_first, seg_last))

    def send_state(k, dx, dc):
        dev = (z, lax.rem(x + dx, nx), lax.rem(c + dc, nc), y)
        return remote(
            states.at[spot], states.at[spot], state_sem.at[0, k], state_sem.at[1, spot], dev
        )

    pl.semaphore_wait(barrier, len(partners))

    state_sends = [send_state(k, k // nc, k % nc) for k in range(1, plane)]
    for copy in state_sends:
        copy.start()
    on_line(0, range(nz), start, late=(False,))
    half = wout_far.shape[0] // nc

    def wout_rows(cc):
        return pl.ds(pl.multiple_of(cc * half, half), half)

    send_wout = remote(
        w_out_ref.at[wout_rows(c)], wout_far.at[wout_rows(c)], wout_sem.at[0], wout_sem.at[1], y_dev
    )
    pass_wout = remote(
        wout_far.at[wout_rows(c)], wout_far.at[wout_rows(c)], wout_sem.at[2], wout_sem.at[3], c_dev
    )
    send_wout.start()
    for b in range(SUBS):
        send_c(0, 0, z, False, b).start()
    for b in range(SUBS):
        send_x(0, 0, z, b).start()
    send_x(1, 0, z, 0).start()

    row_ids = lax.broadcasted_iota(jnp.int32, (rows, rows), 0)
    col_ids = lax.broadcasted_iota(jnp.int32, (rows, rows), 1)
    allowed = (col_ids <= row_ids) & (seg_col == seg_row)
    inner = []
    for p in range(pairs):
        span = pl.ds(p * lanes, lanes)
        queries = query_ref[:, span] * jnp.asarray(hd**-0.5, jnp.bfloat16)
        keys = key_ref[:, span]
        values = value_ref[:, span]
        zero = jnp.zeros_like(queries)
        peaks, sums, outs = [], [], []
        for i in range(2):
            h = 2 * p + i
            mine = near if i == 0 else jnp.logical_not(near)
            scores = dot(jnp.where(mine, queries, zero), keys, NT)
            cum_col = columns[:, heads + h : heads + h + 1]
            inside = jnp.where(
                allowed, cum_col - cum_row[h : h + 1] + in_row[h : h + 1], very_negative
            )
            peak = jnp.max(inside, axis=1, keepdims=True)
            weight = jnp.exp(inside - peak) * scores
            peaks.append(peak)
            sums.append(jnp.sum(weight, axis=1, keepdims=True))
            outs.append(dot(weight.astype(jnp.bfloat16), jnp.where(mine, values, zero)))
        cum_pair = jnp.where(
            near,
            columns[:, heads + 2 * p : heads + 2 * p + 1],
            columns[:, heads + 2 * p + 1 : heads + 2 * p + 2],
        )
        inner.append(
            (
                queries,
                cum_pair,
                jnp.where(near, peaks[0], peaks[1]),
                jnp.where(near, sums[0], sums[1]),
                outs[0] + outs[1],
            )
        )

    def load(ref, i, p):
        info = ref[i, p * tall + hd : (p + 1) * tall, :]
        return (ref[i, p * tall : p * tall + hd, :],) + tuple(info[j : j + 1] for j in range(5))

    def empty():
        zero = jnp.zeros((1, lanes), jnp.float32)
        return (
            jnp.zeros((hd, lanes), jnp.float32),
            zero,
            zero + very_negative,
            zero,
            zero - 1.0,
            zero - 1.0,
        )

    for dx in range(nx):
        for dc in range(nc):
            if dx or dc:
                other = lax.rem(x + dx, nx) * nc + lax.rem(c + dc, nc)
                remote(
                    states.at[other],
                    states.at[other],
                    state_sem.at[0, dx * nc + dc],
                    state_sem.at[1, other],
                    c_dev,
                ).wait_recv()
    prefix = []
    for p in range(pairs):
        so_far = load(states, 0, p)
        mine = choose(spot == 0, empty(), so_far)
        for i in range(1, plane):
            if i > 1:
                mine = choose(spot == i, so_far, mine)
            so_far = combine_rows(so_far, load(states, i, p))
        prefix.append(mine)
        store(totals, 0, p, so_far)

    back = before.shape[0]

    def send_total(d):
        return remote(
            totals.at[0],
            before.at[d - 1],
            total_sem.at[0, d - 1],
            total_sem.at[1, d - 1],
            (lax.rem(z + d, nz), x, c, y),
        )

    for d in range(back, 0, -1):
        pl.when(z + d < nz)(lambda d=d: send_total(d).start())
    on_line(0, range(nz), start, late=(True,))

    for d in range(1, back + 1):
        pl.when(z >= d)(lambda d=d: send_total(d).wait_recv())

        @pl.when(z < d)
        def _(d=d):
            for p in range(pairs):
                store(before, d - 1, p, empty())

    wide_near = lax.broadcasted_iota(jnp.int32, (lanes, lanes), 1) < hd
    wide_top = lax.broadcasted_iota(jnp.int32, (lanes, lanes), 0) < hd
    block = wide_near == wide_top
    for p in range(pairs):
        queries, cum_pair, peak_in, sum_in, from_block = inner[p]
        incoming = load(before, back - 1, p)
        for d in range(back - 1, 0, -1):
            incoming = combine_rows(incoming, load(before, d - 1, p))
        memory, normal, top_row, _, _, last_row = combine_rows(incoming, prefix[p])
        outside = jnp.where(seg_col == last_row, cum_pair + top_row, very_negative)
        peak = jnp.maximum(outside, peak_in)
        carried = jnp.exp(outside - peak)
        inside = jnp.exp(peak_in - peak)
        keep = jnp.where(block, jnp.concatenate([memory, memory], axis=0), 0.0)
        norms = jnp.where(block, jnp.broadcast_to(normal, (lanes, lanes)), 0.0)
        both = jnp.concatenate([keep, norms], axis=0)
        readout = sum(dot(queries, piece, NT) for piece in thirds(both))
        numer = carried * readout[:, :lanes] + inside * from_block
        denom = carried * readout[:, lanes:] + inside * sum_in
        mixed = numer / jnp.maximum(jnp.abs(denom), jnp.exp(-peak))
        mixed_buf[:, p * lanes : (p + 1) * lanes] = mixed.astype(jnp.bfloat16)

    far_rows = pl.ds(pl.multiple_of((1 - y) * own, own), own)
    own_rows = pl.ds(pl.multiple_of(y * own, own), own)
    send_mixed = remote(mixed_buf.at[far_rows], mixed_far, mix_sem.at[0], mix_sem.at[1], y_dev)
    send_mixed.start()

    def relay_near(m, k, b):
        arrived(m, order[k], x, c, b)
        if k > 1:
            on_relay(m, k, b, start)
        send_x(m, k, order[k], b).start()
        send_c(m, k, order[k], False, b).start()

    def relay_far(m, k, b):
        arrived(m, order[k], 1 - x, c, b)
        send_c(m, k, order[k], True, b).start()

    subs = range(SUBS)
    @pl.when(inside_line)
    def _():
        for b in subs[:2]:
            relay_near(0, 2, b)

    load_residual.wait()
    load_wout.wait()
    projected = dot(mixed_buf[own_rows, :], wout_own[...])
    send_wout.wait_recv()
    pass_wout.start()
    send_mixed.wait_recv()
    remote(
        wout_far.at[wout_rows(1 - c)],
        wout_far.at[wout_rows(1 - c)],
        wout_sem.at[2],
        wout_sem.at[3],
        c_dev,
    ).wait_recv()
    projected = projected + dot(mixed_far[...], wout_far[...])
    middle = (residual_buf[...].astype(jnp.float32) + projected).astype(jnp.bfloat16)
    middle_buf[...] = middle
    wide = middle.astype(jnp.float32)
    factor = lax.rsqrt(jnp.mean(wide * wide, axis=-1, keepdims=True) + epsilon)
    gain = gain_ref[...].astype(jnp.float32).reshape(1, model)
    gathered[0:own, :] = (wide * factor * gain).astype(jnp.bfloat16)

    part = own // 2

    def give(kind, h):
        src, dst, dev = ((0, 2, n_dev), (0, 1, y_dev), (2, 3, y_dev))[kind]
        return remote(
            gathered.at[pl.ds(src * own + h * part, part)],
            gathered.at[pl.ds(dst * own + h * part, part)],
            gather_sem.at[0, kind, h],
            gather_sem.at[1, dst - 1, h],
            dev,
        )

    for h in range(2):
        give(0, h).start()
    for h in range(2):
        give(1, h).start()

    def take(h):
        give(0, h).wait_recv()
        give(2, h).start()

    for b in subs:
        relay_near(0, 1, b)
    pl.when(jnp.logical_not(inside_line))(lambda: [relay_near(0, 2, b) for b in subs[:2]] and None)
    for b in subs[2:]:
        relay_near(0, 2, b)
    on_line(1, ends, start)
    for b in subs:
        send_c(1, 0, z, False, b).start()
    for b in range(1, SUBS):
        send_x(1, 0, z, b).start()
    for b in subs:
        relay_near(0, nz - 1, b)
    for h in range(2):
        take(h)
    on_line(1, mids, start)
    def nears(m, k):
        for b in subs:
            relay_near(m, k, b)

    def fars(m, k):
        for b in subs:
            relay_far(m, k, b)

    for k in range(nz - 1):
        fars(0, k)
    nears(1, 1)
    fars(0, nz - 1)

    for m in range(2):
        for b in subs:
            local(m, b).wait()
    for s in order:
        for xx in range(nx):
            for b in subs:
                arrived(0, s, lax.rem(x + xx, nx), 1 - c, b)
    for h in range(2):
        give(1, h).wait_recv()
        give(2, h).wait_recv()

    pl.when(inside_line)(lambda: nears(1, 3))
    def lift(i, carry):
        at_units = pl.ds(pl.multiple_of(i * tile, tile), tile)
        lifted = dot(gathered[...], up_buf[:, at_units])
        positive = jnp.maximum(lifted, 0.0)
        hidden[:, at_units] = (positive * positive).astype(jnp.bfloat16)
        return carry

    lax.fori_loop(0, units // tile, lift, 0)

    def send_part_y(j):
        return remote(
            part_y.at[j], part_y_far.at[j], part_y_sem.at[0, j], part_y_sem.at[1, j], y_dev
        )

    def send_part_z(j):
        return remote(
            part_z.at[j], part_z_far.at[j], part_z_sem.at[0, j], part_z_sem.at[1, j], n_dev
        )

    def lower(k, dx):
        s, xx = order[k], lax.rem(x + dx, nx)
        j = s * nx + xx
        for b in subs:
            arrived(1, s, xx, 1 - c, b)
        terms = dot(hidden[...], down_buf[j])
        for dz in range(PAIR):
            first = dz * ny * own
            part_own[j, dz] = terms[first : first + own]
            part_y[j, dz] = terms[first + own : first + 2 * own].astype(jnp.bfloat16)
        send_part_y(j).start()

    def pass_on(k, dx):
        j = order[k] * nx + lax.rem(x + dx, nx)
        send_part_y(j).wait_recv()
        summed = part_own[j, 1] + part_y_far[j, 1].astype(jnp.float32)
        part_z[j] = summed.astype(jnp.bfloat16)
        send_part_z(j).start()

    def put_out(j):
        at_cols = pl.ds(pl.multiple_of(j * tile, tile), tile)
        return pltpu.make_async_copy(out_buf.at[:, at_cols], out_ref.at[:, at_cols], out_sem.at[j])

    def finish(k, dx):
        j = order[k] * nx + lax.rem(x + dx, nx)
        send_part_z(j).wait_recv()
        at_cols = pl.ds(pl.multiple_of(j * tile, tile), tile)
        summed = part_own[j, 0] + part_y_far[j, 0].astype(jnp.float32)
        summed = summed + part_z_far[j].astype(jnp.float32)
        out_buf[:, at_cols] = (middle_buf[:, at_cols].astype(jnp.float32) + summed).astype(
            jnp.bfloat16
        )
        put_out(j).start()

    def over_x(what, k):
        def one(i, carry):
            what(k, i)
            return carry

        lax.fori_loop(0, nx, one, 0)

    pl.when(inside_line)(lambda: nears(1, 2))

    def at_ends(k, bs):
        @pl.when(jnp.logical_not(inside_line))
        def _():
            for b in bs:
                relay_near(1, k, b)

    at_ends(3, subs)
    fars(1, 0)
    over_x(lower, 0)
    at_ends(2, subs[:1])
    fars(1, 1)
    lower(1, 0)
    at_ends(2, subs[1:2])
    lower(1, 1)
    at_ends(2, subs[2:3])
    over_x(pass_on, 0)
    at_ends(2, subs[3:])
    fars(1, 3)
    lower(3, 0)
    over_x(pass_on, 1)
    lower(3, 1)
    fars(1, 2)
    lower(2, 0)
    over_x(pass_on, 3)
    lower(2, 1)
    pass_on(2, 0)
    pass_on(2, 1)
    for k in (0, 1, 3, 2):
        over_x(finish, k)

    def put(j, carry):
        put_out(j).wait()
        return carry

    lax.fori_loop(0, nz * nx, put, 0)

    wait = lambda copy: copy.wait_send()
    for m in range(2):
        on_line(m, range(nz), wait)
        for k in range(nz):
            for b in subs:
                if k > 1:
                    on_relay(m, k, b, wait)
                wait(send_x(m, k, order[k], b))
                wait(send_c(m, k, order[k], False, b))
                wait(send_c(m, k, order[k], True, b))
    for copy in state_sends + [send_wout, pass_wout, send_mixed]:
        wait(copy)
    for kind in range(3):
        for h in range(2):
            wait(give(kind, h))
    for d in range(1, back + 1):
        pl.when(z + d < nz)(lambda d=d: send_total(d).wait_send())

    def drained(j, carry):
        wait(send_part_y(j))
        wait(send_part_z(j))
        return carry

    lax.fori_loop(0, nz * nx, drained, 0)


def fused(
    residual,
    query_vectors,
    key_vectors,
    value_vectors,
    in_gate,
    forget_gate,
    documents,
    w_out,
    norm_gain,
    w_up,
    w_down,
):
    sizes = tuple(lax.axis_size(name) for name in ("z", "x", "c", "tp"))
    nz, nx, nc, ny = sizes
    rows, width = query_vectors.shape
    heads = in_gate.shape[0]
    own, model = residual.shape
    depth, cols = w_up.shape[0], w_down.shape[1]
    units = w_up.shape[1] // PAIR
    members = PAIR * ny
    plane = nx * nc
    pairs = heads // 2
    state = (pairs * (width // heads + 8), width // pairs)
    reach = min(nz * plane - 1, -(-(DOC_MOST - 1) // rows))
    back = -(-reach // plane)
    bf16, f32 = jnp.bfloat16, jnp.float32
    dma = pltpu.SemaphoreType.DMA
    vmem = pl.BlockSpec(memory_space=pltpu.VMEM)
    anywhere = pl.BlockSpec(memory_space=pl.ANY)
    return pl.pallas_call(
        functools.partial(layer_kernel, sizes),
        out_shape=jax.ShapeDtypeStruct((own, model), bf16),
        in_specs=[vmem] * 7 + [anywhere] * 4,
        out_specs=anywhere,
        scratch_shapes=[
            pltpu.VMEM((nz * plane * depth, units), bf16),
            pltpu.VMEM((nz * nx, units, nc * cols), bf16),
            pltpu.VMEM(w_out.shape, bf16),
            pltpu.VMEM(w_out.shape, bf16),
            pltpu.VMEM((own, model), bf16),
            pltpu.VMEM((plane,) + state, f32),
            pltpu.VMEM((1,) + state, f32),
            pltpu.VMEM((back,) + state, f32),
            pltpu.VMEM((rows, width), bf16),
            pltpu.VMEM((own, width), bf16),
            pltpu.VMEM((members * own, model), bf16),
            pltpu.VMEM((members * own, units), bf16),
            pltpu.VMEM((own, model), bf16),
            pltpu.VMEM((nz * nx, PAIR, own, nc * cols), f32),
            pltpu.VMEM((nz * nx, PAIR, own, nc * cols), bf16),
            pltpu.VMEM((nz * nx, PAIR, own, nc * cols), bf16),
            pltpu.VMEM((nz * nx, own, nc * cols), bf16),
            pltpu.VMEM((nz * nx, own, nc * cols), bf16),
            pltpu.VMEM((own, model), bf16),
            dma((2, nz * plane, SUBS)),
            dma((2, 4, SUBS)),
            dma((2, nz, SUBS)),
            dma((2, nz, 2, SUBS)),
            dma((3, SUBS)),
            dma((2, plane)),
            dma((2, back)),
            dma((2,)),
            dma((4,)),
            dma((2, 3, 2)),
            dma((2, nz * nx)),
            dma((2, nz * nx)),
            dma((nz * nx,)),
        ],
        compiler_params=pltpu.CompilerParams(
            collective_id=0, has_side_effects=True, vmem_limit_bytes=60 * 1024 * 1024
        ),
    )(
        query_vectors,
        key_vectors,
        value_vectors,
        in_gate,
        forget_gate,
        documents.reshape(1, rows),
        norm_gain,
        residual,
        w_out,
        w_up,
        w_down,
    )


def suits(shape, args):
    nz, nx, nc, ny = shape
    query_vectors, in_gate, w_up, w_down = args[1], args[4], args[9], args[10]
    total, width = query_vectors.shape
    depth, cols = w_up.shape[0] // (nz * nx * nc), w_down.shape[1] // (nz * nx * nc)
    heads = in_gate.shape[0] // ny
    return (
        (nz, nx, nc, ny) == (2 * PAIR, 2, 2, 2)
        and depth % 128 == 0
        and cols % 128 == 0
        and heads == 4
        and width // in_gate.shape[0] == 64
        and total // (nz * nx * nc) == 256
    )


def solution(mesh):
    sp, tp = mesh.shape["sp"], mesh.shape["tp"]
    chips = tp if sp % (2 * tp) == 0 else 1
    cores = 2 if sp % 2 == 0 else 1
    shape = (sp // (chips * cores), chips, cores, tp)
    split = Mesh(np.asarray(mesh.devices).reshape(shape), ("z", "x", "c", "tp"))
    placed = (
        P(("z", "x", "c", "tp"), None),
        P(SP, "tp"),
        P(SP, "tp"),
        P(SP, "tp"),
        P("tp", SP),
        P("tp", SP),
        P(SP),
        P("tp", None),
        P(),
        P(SP, "tp"),
        P("tp", SP),
    )

    def run(*args):
        return jax.shard_map(
            fused if suits(shape, args) else on_device,
            mesh=split,
            in_specs=placed,
            out_specs=P(("z", "x", "c", "tp"), None),
            check_vma=False,
        )(*args)

    return run
```

```python
import functools

import jax
import jax.numpy as jnp
import numpy as np
from jax import lax
from jax.experimental import pallas as pl
from jax.experimental.pallas import tpu as pltpu
from jax.sharding import Mesh, PartitionSpec as P

DOC_MOST = 2048
very_negative = -1e30
epsilon = 1e-06
SP = ("z", "x", "c")
G = ("x", "c")


def combine(earlier, later):
    memory_one, top_one, decay_one, first_one, last_one = earlier
    memory_two, top_two, decay_two, first_two, last_two = later
    later_empty = first_two < 0.0
    earlier_empty = first_one < 0.0
    keep = later_empty | (first_two == last_two) & (first_two == last_one)
    decay_step = jnp.where(later_empty, 0.0, decay_two)
    top_new = jnp.where(keep, jnp.maximum(decay_step + top_one, top_two), top_two)
    scale_old = jnp.where(keep, jnp.exp(decay_step + top_one - top_new), 0.0)
    scale_new = jnp.exp(top_two - top_new)
    memory_new = scale_old[:, None, None] * memory_one + scale_new[:, None, None] * memory_two
    decay_new = jnp.where(keep, decay_one + decay_step, decay_two)
    first_new = jnp.where(earlier_empty, first_two, first_one)
    last_new = jnp.where(later_empty, last_one, last_two)
    return (memory_new, top_new, decay_new, first_new, last_new)


def pack(state):
    memory, top, decay, first, last = state
    heads, _, width = memory.shape
    row = jnp.stack(
        [top, decay, jnp.broadcast_to(first, top.shape), jnp.broadcast_to(last, top.shape)], axis=1
    )
    row = jnp.pad(row, ((0, 0), (0, width - 4)))
    return jnp.concatenate(
        [memory, row[:, None, :], jnp.zeros((heads, 6, width), jnp.float32)], axis=1
    )


def unpack(packed, present):
    rows = packed.shape[1] - 7
    row = packed[:, rows]
    memory = jnp.where(present, packed[:, :rows], 0.0)
    top = jnp.where(present, row[:, 0], very_negative)
    decay = jnp.where(present, row[:, 1], 0.0)
    first = jnp.where(present, row[0, 2], -1.0)
    last = jnp.where(present, row[0, 3], -1.0)
    return (memory, top, decay, first, last)


def shifted(state, distance, length, here):
    packed = lax.ppermute(pack(state), SP, [(i, i + distance) for i in range(length - distance)])
    return unpack(packed, here >= distance)


def turn(value, axis, d):
    n = lax.axis_size(axis)
    return lax.ppermute(value, axis, [(i, (i + d) % n) for i in range(n)])


def reduced(terms, dim, axis):
    def block(d):
        return lax.index_in_dim(terms, d, dim, keepdims=False)

    total = block(0).astype(jnp.float32)
    for d in range(1, lax.axis_size(axis)):
        total = total + turn(block(d), axis, -d).astype(jnp.float32)
    return total.astype(jnp.bfloat16)


def on_device(
    residual,
    query_vectors,
    key_vectors,
    value_vectors,
    in_gate,
    forget_gate,
    documents,
    w_out,
    norm_gain,
    w_up,
    w_down,
):
    tok_rows = query_vectors.shape[0]
    heads = in_gate.shape[0]
    head_dim = query_vectors.shape[1] // heads
    length = lax.axis_size(SP)
    here = lax.axis_index(SP)
    tp = lax.axis_size("tp")
    me = lax.axis_index("tp")

    plane = lax.axis_size(G)
    up_pieces = jnp.transpose(w_up.reshape(w_up.shape[0], plane, -1), (1, 0, 2))
    up_part = lax.all_to_all(up_pieces, G, split_axis=0, concat_axis=0, tiled=True)
    up_part = up_part.reshape(-1, up_part.shape[-1])
    up_part, w_down, w_out, key_vectors, in_gate, forget_gate, documents = (
        lax.optimization_barrier(
            (up_part, w_down, w_out, key_vectors, in_gate, forget_gate, documents)
        )
    )
    down_part = lax.all_to_all(w_down, G, split_axis=0, concat_axis=1, tiled=True)
    up_all = lax.all_gather(up_part, "z", axis=0, tiled=True)
    down_all = lax.all_gather(down_part, "z", axis=1, tiled=True)

    w_out_parts = [w_out] + [turn(w_out, "tp", d) for d in range(1, tp)]

    segment = documents.astype(jnp.float32)
    decay_log = jax.nn.log_sigmoid(forget_gate)
    cumulative = jnp.cumsum(decay_log, axis=-1)
    key_heads = jnp.transpose(key_vectors.reshape(tok_rows, heads, head_dim), (1, 0, 2))
    value_heads = jnp.transpose(value_vectors.reshape(tok_rows, heads, head_dim), (1, 0, 2))
    query_heads = jnp.transpose(query_vectors.reshape(tok_rows, heads, head_dim), (1, 0, 2))
    query_heads = query_heads * jnp.asarray(head_dim ** (-0.5), query_heads.dtype)
    latest = segment == segment[-1]
    growth = jnp.where(latest[None, :], cumulative[:, -1:] - cumulative + in_gate, very_negative)
    top_log = jnp.max(growth, axis=-1)
    summary_weight = jnp.exp(growth - top_log[:, None])
    key_wide = key_heads.astype(jnp.float32)
    weighted = key_wide * summary_weight[:, :, None]
    memory = jnp.einsum(
        "hsv,hsk->hvk", value_heads.astype(jnp.float32), weighted, precision=lax.Precision.HIGHEST
    )
    normal = jnp.sum(weighted, axis=1)
    state = (
        jnp.concatenate([memory, normal[:, None, :]], axis=1),
        top_log,
        cumulative[:, -1],
        segment[0],
        segment[-1],
    )

    reach = min(length - 1, -(-(DOC_MOST - 1) // tok_rows))
    span = 1
    while span < reach:
        state = combine(shifted(state, span, length, here), state)
        span *= 2
    incoming = shifted(state, 1, length, here)
    memory_in, top_in, _, _, last_in = incoming

    row_ids = lax.broadcasted_iota(jnp.int32, (tok_rows, tok_rows), 0)
    col_ids = lax.broadcasted_iota(jnp.int32, (tok_rows, tok_rows), 1)
    allowed = (col_ids <= row_ids) & (segment[:, None] == segment[None, :])
    inside = jnp.where(
        allowed[None],
        cumulative[:, :, None] - cumulative[:, None, :] + in_gate[:, None, :],
        very_negative,
    )
    peak_inside = jnp.max(inside, axis=-1)
    scores = jnp.einsum(
        "hld,hsd->hls", query_heads, key_heads, preferred_element_type=jnp.float32
    )
    weight_inside = jnp.exp(inside - peak_inside[:, :, None]) * scores
    from_block = jnp.einsum(
        "hls,hsv->hlv",
        weight_inside.astype(jnp.bfloat16),
        value_heads,
        preferred_element_type=jnp.float32,
    )
    sum_inside = jnp.sum(weight_inside, axis=-1)

    outside = jnp.where((segment == last_in)[None, :], cumulative + top_in[:, None], very_negative)
    peak_log = jnp.maximum(outside, peak_inside)
    carried = jnp.exp(outside - peak_log)
    local = jnp.exp(peak_inside - peak_log)
    readout = jnp.einsum(
        "hlk,hvk->hlv",
        query_heads.astype(jnp.float32),
        memory_in,
        precision=lax.Precision.HIGHEST,
    )
    numer = carried[:, :, None] * readout[:, :, :head_dim] + local[:, :, None] * from_block
    denom = carried * readout[:, :, head_dim] + local * sum_inside
    mixed = numer / jnp.maximum(jnp.abs(denom), jnp.exp(-peak_log))[:, :, None]
    mixed = jnp.transpose(mixed, (1, 0, 2)).reshape(tok_rows, -1).astype(jnp.bfloat16)

    own_rows = tok_rows // tp
    mixed_rows = mixed.reshape(tp, own_rows, -1)
    projected = 0.0
    for d in range(tp):
        piece = lax.dynamic_index_in_dim(mixed_rows, (me + d) % tp, 0, keepdims=False)
        if d:
            piece = turn(piece, "tp", d)
        projected = projected + jnp.dot(
            piece, w_out_parts[d], preferred_element_type=jnp.float32
        )
    middle = (residual.astype(jnp.float32) + projected).astype(jnp.bfloat16)
    middle_wide = middle.astype(jnp.float32)
    factor = lax.rsqrt(jnp.mean(middle_wide * middle_wide, axis=-1, keepdims=True) + epsilon)
    normed = (middle_wide * factor * norm_gain.astype(jnp.float32)).astype(jnp.bfloat16)

    gathered = normed
    for axis in ("tp", "x", "c"):
        gathered = jnp.concatenate(
            [gathered] + [turn(gathered, axis, d) for d in range(1, lax.axis_size(axis))], axis=0
        )
    lifted = jnp.dot(gathered, up_all, preferred_element_type=jnp.float32)
    hidden = jnp.square(jax.nn.relu(lifted)).astype(jnp.bfloat16)
    sizes = (lax.axis_size("c"), lax.axis_size("x"), tp)
    half = down_all.shape[1] // 2
    summed = []
    for k, order in enumerate((("c", "x", "tp"), ("c", "tp", "x"))):
        terms = jnp.dot(
            hidden, down_all[:, k * half : (k + 1) * half], preferred_element_type=jnp.float32
        )
        terms = terms.astype(jnp.bfloat16).reshape(*sizes, own_rows, half)
        names = ["c", "x", "tp"]
        for axis in order:
            terms = reduced(terms, names.index(axis), axis)
            names.remove(axis)
        summed.append(terms.astype(jnp.float32))
    return (middle_wide + jnp.concatenate(summed, axis=1)).astype(jnp.bfloat16)


MESH = pl.DeviceIdType.MESH
PAIR = 2
SUBS = 4
NT = (((1,), (1,)), ((), ()))
NN = (((1,), (0,)), ((), ()))


def dot(a, b, dims=NN):
    return lax.dot_general(a, b, dims, preferred_element_type=jnp.float32)


def thirds(value):
    high = value.astype(jnp.bfloat16)
    rest = value - high.astype(jnp.float32)
    middle = rest.astype(jnp.bfloat16)
    low = (rest - middle.astype(jnp.float32)).astype(jnp.bfloat16)
    return high, middle, low


def combine_rows(earlier, later):
    memory_one, normal_one, top_one, decay_one, first_one, last_one = earlier
    memory_two, normal_two, top_two, decay_two, first_two, last_two = later
    later_empty = first_two < 0.0
    earlier_empty = first_one < 0.0
    keep = later_empty | (first_two == last_two) & (first_two == last_one)
    decay_step = jnp.where(later_empty, 0.0, decay_two)
    top_new = jnp.where(keep, jnp.maximum(decay_step + top_one, top_two), top_two)
    scale_old = jnp.where(keep, jnp.exp(decay_step + top_one - top_new), 0.0)
    scale_new = jnp.exp(top_two - top_new)
    return (
        scale_old * memory_one + scale_new * memory_two,
        scale_old * normal_one + scale_new * normal_two,
        top_new,
        jnp.where(keep, decay_one + decay_step, decay_two),
        jnp.where(earlier_empty, first_two, first_one),
        jnp.where(later_empty, last_one, last_two),
    )


def choose(flag, one, two):
    return tuple(jnp.where(flag, a, b) for a, b in zip(one, two))


def layer_kernel(
    sizes,
    query_ref,
    key_ref,
    value_ref,
    in_ref,
    forget_ref,
    document_ref,
    gain_ref,
    residual_ref,
    w_out_ref,
    w_up_ref,
    w_down_ref,
    out_ref,
    up_buf,
    down_buf,
    wout_own,
    wout_far,
    residual_buf,
    states,
    totals,
    before,
    mixed_buf,
    mixed_far,
    gathered,
    hidden,
    middle_buf,
    part_own,
    part_y,
    part_y_far,
    part_z,
    part_z_far,
    out_buf,
    line_sem,
    far_sem,
    core_sem,
    sent,
    local_sem,
    state_sem,
    total_sem,
    mix_sem,
    wout_sem,
    gather_sem,
    part_y_sem,
    part_z_sem,
):
    nz, nx, nc, ny = sizes
    z, x, c, y = (lax.axis_index(name) for name in ("z", "x", "c", "tp"))
    zl = z // PAIR
    zn = lax.rem(z + PAIR, nz)
    rows, width = query_ref.shape
    heads = in_ref.shape[0]
    pairs = heads // 2
    lanes = width // pairs
    hd = lanes // 2
    own = rows // ny
    model = out_ref.shape[1]
    depth = w_up_ref.shape[0]
    cols = w_down_ref.shape[1]
    units = w_up_ref.shape[1] // PAIR
    sub = units // SUBS
    plane = nx * nc
    spot = x * nc + c
    tile = nc * cols

    def remote(src, dst, send, recv, dev):
        return pltpu.make_async_remote_copy(
            src_ref=src,
            dst_ref=dst,
            send_sem=send,
            recv_sem=recv,
            device_id=dev,
            device_id_type=MESH,
        )

    x_dev = (z, 1 - x, c, y)
    c_dev = (z, x, 1 - c, y)
    y_dev = (z, x, c, 1 - y)
    n_dev = (zn, x, c, y)

    def place(s, xx, cc):
        return (s * nx + xx) * nc + cc

    def slot(m, s, xx, cc, b):
        if m == 0:
            start = pl.multiple_of(place(s, xx, cc) * depth, depth)
            return up_buf.at[pl.ds(start, depth), pl.ds(b * sub, sub)]
        lane0 = pl.multiple_of(cc * cols, cols)
        return down_buf.at[s * nx + xx, pl.ds(b * sub, sub), pl.ds(lane0, cols)]

    def source(m, g, b):
        start = pl.multiple_of(g * units + b * sub, sub)
        if m == 0:
            return w_up_ref.at[:, pl.ds(start, sub)]
        return w_down_ref.at[pl.ds(start, sub), :]

    def send_z(m, g, s, to, b):
        src = source(m, g, b) if s is None else slot(m, s, x, c, b)
        s = z if s is None else s
        return remote(
            src,
            slot(m, s, x, c, b),
            sent.at[0],
            line_sem.at[m, s, b],
            (jnp.int32(to), x, c, y),
        )

    def send_x(m, k, s, b):
        src = source(m, zl, b) if k == 0 else slot(m, s, x, c, b)
        return remote(src, slot(m, s, x, c, b), sent.at[1], far_sem.at[m, s, b], x_dev)

    def send_c(m, k, s, far, b):
        xx = 1 - x if far else x
        src = source(m, zl, b) if k == 0 and not far else slot(m, s, xx, c, b)
        return remote(src, slot(m, s, xx, c, b), sent.at[2], core_sem.at[m, s, xx], c_dev)

    def arrived(m, s, xx, b, sem):
        here = slot(m, s, xx, c, b)
        remote(here, here, sent.at[1], sem.at[m, s, b], x_dev).wait_recv()

    def shared(m, s, xx):
        start = pl.multiple_of(place(s, xx, 1 - c) * depth, depth)
        lane0 = pl.multiple_of((1 - c) * cols, cols)
        here = (
            up_buf.at[pl.ds(start, depth), :],
            down_buf.at[s * nx + xx, :, pl.ds(lane0, cols)],
        )[m]
        remote(here, here, sent.at[2], core_sem.at[m, s, xx], c_dev).wait_recv()

    def local(m, b):
        return pltpu.make_async_copy(source(m, zl, b), slot(m, z, x, c, b), local_sem.at[0])

    def all_left(kind, like):
        pltpu.make_async_copy(like, like, sent.at[kind]).wait()

    to_left = {1: [(0, 0)], 2: [(0, 1)], 3: [(1, 2), (0, 1)]}
    to_right = {0: [(0, 1), (1, 2)], 1: [(1, 2)], 2: [(1, 3)]}

    def on_line(m, places, act, late=(False, True)):
        for kz in places:
            lefts, rights = to_left.get(kz, []), to_right.get(kz, [])
            todo = []
            for i, (g, to) in enumerate(lefts + rights):
                for b in range(SUBS):
                    behind = i > len(lefts) or (i == len(lefts) and b >= ahead[kz])
                    if behind in late:
                        todo.append((i, g, to, b))

            @pl.when(z == kz)
            def _(todo=todo):
                for i, g, to, b in todo:
                    act(send_z(m, g, None, to, b))

    ends, mids = (0, nz - 1), tuple(range(1, nz - 1))
    ahead = (1, 2, 2, 0)
    inside_line = (z > 0) & (z < nz - 1)

    def on_relay(m, k, b, act):
        for kz, to in ((1, 0), (2, 3)):
            pl.when(z == kz)(lambda to=to: act(send_z(m, None, order[k], to, b)))

    start = lambda copy: copy.start()
    order = [z, z + 1 - 2 * lax.rem(z, PAIR), 2 - z // 2, (nz - 1) * (1 - z // 2)]

    barrier = pltpu.get_barrier_semaphore()
    partners = [(lax.rem(z + d, nz), x, c, y) for d in range(1, nz)]
    partners += [x_dev, c_dev, (z, 1 - x, 1 - c, y), y_dev]
    for dev in partners:
        pl.semaphore_signal(barrier, inc=1, device_id=dev, device_id_type=MESH)

    load_residual = pltpu.make_async_copy(residual_ref, residual_buf, local_sem.at[1])
    load_wout = pltpu.make_async_copy(w_out_ref, wout_own, local_sem.at[2])
    load_residual.start()
    load_wout.start()
    for m in range(2):
        for b in range(SUBS):
            local(m, b).start()

    near = lax.broadcasted_iota(jnp.int32, (1, lanes), 1) < hd
    forget = forget_ref[...]
    decay_log = jnp.minimum(forget, 0.0) - jnp.log1p(jnp.exp(-jnp.abs(forget)))
    gates = jnp.concatenate([decay_log, in_ref[...]], axis=0)
    at = lax.broadcasted_iota(jnp.int32, gates.shape, 1)
    running = gates
    step = 1
    while step < rows:
        running = running + jnp.where(at >= step, pltpu.roll(running, step, 1), 0.0)
        step *= 2
    cum_row = running[:heads]
    in_row = gates[heads:]
    seg_row = document_ref[...].astype(jnp.float32)
    seg_first = seg_row[:, 0:1]
    seg_last = seg_row[:, rows - 1 : rows]
    total = cum_row[:, rows - 1 : rows]
    growth = jnp.where(seg_row == seg_last, total - cum_row + in_row, very_negative)
    top = jnp.max(growth, axis=1, keepdims=True)
    summary = jnp.exp(growth - top)
    columns = jnp.transpose(jnp.concatenate([summary, cum_row], axis=0))
    seg_col = jnp.transpose(jnp.broadcast_to(seg_row, (2 * heads, rows)))[:, 0:1]

    row_of = lax.broadcasted_iota(jnp.int32, (8, lanes), 0)
    tall = hd + 8

    def store(ref, i, p, state):
        info = jnp.zeros((8, lanes), jnp.float32)
        for j, line in enumerate(state[1:]):
            info = jnp.where(row_of == j, line, info)
        ref[i, p * tall : p * tall + hd, :] = state[0]
        ref[i, p * tall + hd : (p + 1) * tall, :] = info

    for p in range(pairs):
        a, b = 2 * p, 2 * p + 1
        span = pl.ds(p * lanes, lanes)
        keys = key_ref[:, span].astype(jnp.float32)
        weighted = keys * jnp.where(near, columns[:, a : a + 1], columns[:, b : b + 1])
        values_t = jnp.transpose(value_ref[:, span])
        full = sum(dot(values_t, piece) for piece in thirds(weighted))
        memory = jnp.where(near, full[:hd], full[hd:])
        normal = jnp.sum(weighted, axis=0, keepdims=True)
        top_row = jnp.where(near, top[a : a + 1], top[b : b + 1])
        decay_row = jnp.where(near, total[a : a + 1], total[b : b + 1])
        store(states, spot, p, (memory, normal, top_row, decay_row, seg_first, seg_last))

    def send_state(i, dev):
        return remote(states.at[i], states.at[i], sent.at[3], state_sem.at[i], dev)

    pl.semaphore_wait(barrier, len(partners))

    beside, across = spot + 1 - 2 * c, (1 - x) * nc + c
    send_state(spot, x_dev).start()
    send_state(spot, c_dev).start()
    on_line(0, range(nz), start, late=(False,))
    half = wout_far.shape[0] // nc

    def wout_rows(cc):
        return pl.ds(pl.multiple_of(cc * half, half), half)

    send_wout = remote(
        w_out_ref.at[wout_rows(c)], wout_far.at[wout_rows(c)], wout_sem.at[0], wout_sem.at[1], y_dev
    )
    pass_wout = remote(
        wout_far.at[wout_rows(c)], wout_far.at[wout_rows(c)], wout_sem.at[2], wout_sem.at[3], c_dev
    )
    send_wout.start()
    for b in range(SUBS):
        send_c(0, 0, z, False, b).start()
    for b in range(SUBS):
        send_x(0, 0, z, b).start()
    send_x(1, 0, z, 0).start()

    row_ids = lax.broadcasted_iota(jnp.int32, (rows, rows), 0)
    col_ids = lax.broadcasted_iota(jnp.int32, (rows, rows), 1)
    allowed = (col_ids <= row_ids) & (seg_col == seg_row)
    inner = []
    for p in range(pairs):
        span = pl.ds(p * lanes, lanes)
        queries = query_ref[:, span] * jnp.asarray(hd**-0.5, jnp.bfloat16)
        keys = key_ref[:, span]
        values = value_ref[:, span]
        zero = jnp.zeros_like(queries)
        peaks, sums, outs = [], [], []
        for i in range(2):
            h = 2 * p + i
            mine = near if i == 0 else jnp.logical_not(near)
            scores = dot(jnp.where(mine, queries, zero), keys, NT)
            cum_col = columns[:, heads + h : heads + h + 1]
            inside = jnp.where(
                allowed, cum_col - cum_row[h : h + 1] + in_row[h : h + 1], very_negative
            )
            peak = jnp.max(inside, axis=1, keepdims=True)
            weight = jnp.exp(inside - peak) * scores
            peaks.append(peak)
            sums.append(jnp.sum(weight, axis=1, keepdims=True))
            outs.append(dot(weight.astype(jnp.bfloat16), jnp.where(mine, values, zero)))
        cum_pair = jnp.where(
            near,
            columns[:, heads + 2 * p : heads + 2 * p + 1],
            columns[:, heads + 2 * p + 1 : heads + 2 * p + 2],
        )
        inner.append(
            (
                queries,
                cum_pair,
                jnp.where(near, peaks[0], peaks[1]),
                jnp.where(near, sums[0], sums[1]),
                outs[0] + outs[1],
            )
        )

    def load(ref, i, p):
        info = ref[i, p * tall + hd : (p + 1) * tall, :]
        return (ref[i, p * tall : p * tall + hd, :],) + tuple(info[j : j + 1] for j in range(5))

    def empty():
        zero = jnp.zeros((1, lanes), jnp.float32)
        return (
            jnp.zeros((hd, lanes), jnp.float32),
            zero,
            zero + very_negative,
            zero,
            zero - 1.0,
            zero - 1.0,
        )

    send_state(across, x_dev).wait_recv()
    send_state(across, c_dev).start()
    send_state(beside, c_dev).wait_recv()
    send_state(across + 1 - 2 * c, c_dev).wait_recv()
    prefix = []
    for p in range(pairs):
        so_far = load(states, 0, p)
        mine = choose(spot == 0, empty(), so_far)
        for i in range(1, plane):
            if i > 1:
                mine = choose(spot == i, so_far, mine)
            so_far = combine_rows(so_far, load(states, i, p))
        prefix.append(mine)
        store(totals, 0, p, so_far)

    back = before.shape[0]

    def send_total(d):
        return remote(
            totals.at[0],
            before.at[d - 1],
            total_sem.at[0, d - 1],
            total_sem.at[1, d - 1],
            (lax.rem(z + d, nz), x, c, y),
        )

    for d in range(back, 0, -1):
        pl.when(z + d < nz)(lambda d=d: send_total(d).start())
    on_line(0, range(nz), start, late=(True,))

    for d in range(1, back + 1):
        pl.when(z >= d)(lambda d=d: send_total(d).wait_recv())

        @pl.when(z < d)
        def _(d=d):
            for p in range(pairs):
                store(before, d - 1, p, empty())

    wide_near = lax.broadcasted_iota(jnp.int32, (lanes, lanes), 1) < hd
    wide_top = lax.broadcasted_iota(jnp.int32, (lanes, lanes), 0) < hd
    block = wide_near == wide_top
    for p in range(pairs):
        queries, cum_pair, peak_in, sum_in, from_block = inner[p]
        incoming = load(before, back - 1, p)
        for d in range(back - 1, 0, -1):
            incoming = combine_rows(incoming, load(before, d - 1, p))
        memory, normal, top_row, _, _, last_row = combine_rows(incoming, prefix[p])
        outside = jnp.where(seg_col == last_row, cum_pair + top_row, very_negative)
        peak = jnp.maximum(outside, peak_in)
        carried = jnp.exp(outside - peak)
        inside = jnp.exp(peak_in - peak)
        keep = jnp.where(block, jnp.concatenate([memory, memory], axis=0), 0.0)
        norms = jnp.where(block, jnp.broadcast_to(normal, (lanes, lanes)), 0.0)
        both = jnp.concatenate([keep, norms], axis=0)
        readout = sum(dot(queries, piece, NT) for piece in thirds(both))
        numer = carried * readout[:, :lanes] + inside * from_block
        denom = carried * readout[:, lanes:] + inside * sum_in
        mixed = numer / jnp.maximum(jnp.abs(denom), jnp.exp(-peak))
        mixed_buf[:, p * lanes : (p + 1) * lanes] = mixed.astype(jnp.bfloat16)

    far_rows = pl.ds(pl.multiple_of((1 - y) * own, own), own)
    own_rows = pl.ds(pl.multiple_of(y * own, own), own)
    send_mixed = remote(mixed_buf.at[far_rows], mixed_far, mix_sem.at[0], mix_sem.at[1], y_dev)
    send_mixed.start()

    def relay_near(m, k, b):
        arrived(m, order[k], x, b, line_sem)
        if k > 1:
            on_relay(m, k, b, start)
        send_x(m, k, order[k], b).start()
        send_c(m, k, order[k], False, b).start()

    def relay_far(m, k, b):
        arrived(m, order[k], 1 - x, b, far_sem)
        send_c(m, k, order[k], True, b).start()

    subs = range(SUBS)
    @pl.when(inside_line)
    def _():
        for b in subs[:2]:
            relay_near(0, 2, b)

    load_residual.wait()
    load_wout.wait()
    projected = dot(mixed_buf[own_rows, :], wout_own[...])
    send_wout.wait_recv()
    pass_wout.start()
    send_mixed.wait_recv()
    remote(
        wout_far.at[wout_rows(1 - c)],
        wout_far.at[wout_rows(1 - c)],
        wout_sem.at[2],
        wout_sem.at[3],
        c_dev,
    ).wait_recv()
    projected = projected + dot(mixed_far[...], wout_far[...])
    middle = (residual_buf[...].astype(jnp.float32) + projected).astype(jnp.bfloat16)
    middle_buf[...] = middle
    wide = middle.astype(jnp.float32)
    factor = lax.rsqrt(jnp.mean(wide * wide, axis=-1, keepdims=True) + epsilon)
    gain = gain_ref[...].astype(jnp.float32).reshape(1, model)
    gathered[0:own, :] = (wide * factor * gain).astype(jnp.bfloat16)

    part = own // 2

    def give(kind, h):
        src, dst, dev = ((0, 2, n_dev), (0, 1, y_dev), (2, 3, y_dev))[kind]
        return remote(
            gathered.at[pl.ds(src * own + h * part, part)],
            gathered.at[pl.ds(dst * own + h * part, part)],
            sent.at[4],
            gather_sem.at[dst - 1, h],
            dev,
        )

    for h in range(2):
        give(0, h).start()
    for h in range(2):
        give(1, h).start()

    def take(h):
        give(0, h).wait_recv()
        give(2, h).start()

    for b in subs:
        relay_near(0, 1, b)
    pl.when(jnp.logical_not(inside_line))(lambda: [relay_near(0, 2, b) for b in subs[:2]] and None)
    for b in subs[2:]:
        relay_near(0, 2, b)
    on_line(1, ends, start)
    for b in subs:
        send_c(1, 0, z, False, b).start()
    for b in range(1, SUBS):
        send_x(1, 0, z, b).start()
    for b in subs:
        relay_near(0, nz - 1, b)
    for h in range(2):
        take(h)
    on_line(1, mids, start)
    def nears(m, k):
        for b in subs:
            relay_near(m, k, b)

    def fars(m, k):
        for b in subs:
            relay_far(m, k, b)

    for k in range(nz - 1):
        fars(0, k)
    nears(1, 1)
    @pl.when(inside_line)
    def _():
        for b in subs[:-1]:
            relay_near(1, 3, b)

    fars(0, nz - 1)

    here = up_buf.at[pl.ds(0, 2 * depth), :]
    pltpu.make_async_copy(here, here, local_sem.at[0]).wait()
    for s in order:
        for xx in range(nx):
            shared(0, s, lax.rem(x + xx, nx))
    for h in range(2):
        give(1, h).wait_recv()
        give(2, h).wait_recv()

    pl.when(inside_line)(lambda: relay_near(1, 3, SUBS - 1))
    def lift(i, carry):
        at_units = pl.ds(pl.multiple_of(i * tile, tile), tile)
        lifted = dot(gathered[...], up_buf[:, at_units])
        positive = jnp.maximum(lifted, 0.0)
        hidden[:, at_units] = (positive * positive).astype(jnp.bfloat16)
        return carry

    lax.fori_loop(0, units // tile, lift, 0)

    def send_part_y(j, dz):
        return remote(
            part_y.at[j, dz], part_y_far.at[j, dz], sent.at[5], part_y_sem.at[j, dz], y_dev
        )

    def send_part_z(j):
        return remote(part_z.at[j], part_z_far.at[j], sent.at[6], part_z_sem.at[j], n_dev)

    def lower(k, dx):
        s, xx = order[k], lax.rem(x + dx, nx)
        j = s * nx + xx
        shared(1, s, xx)
        terms = dot(hidden[...], down_buf[j])
        for dz in reversed(range(PAIR)):
            first = dz * ny * own
            part_own[j, dz] = terms[first : first + own]
            part_y[j, dz] = terms[first + own : first + 2 * own].astype(jnp.bfloat16)
        for dz in reversed(range(PAIR)):
            send_part_y(j, dz).start()

    def pass_on(k, dx):
        j = order[k] * nx + lax.rem(x + dx, nx)
        send_part_y(j, 1).wait_recv()
        summed = part_own[j, 1] + part_y_far[j, 1].astype(jnp.float32)
        part_z[j] = summed.astype(jnp.bfloat16)
        send_part_z(j).start()

    def put_out(j):
        at_cols = pl.ds(pl.multiple_of(j * tile, tile), tile)
        return pltpu.make_async_copy(out_buf.at[:, at_cols], out_ref.at[:, at_cols], sent.at[7])

    def finish(k, dx):
        j = order[k] * nx + lax.rem(x + dx, nx)
        send_part_y(j, 0).wait_recv()
        send_part_z(j).wait_recv()
        at_cols = pl.ds(pl.multiple_of(j * tile, tile), tile)
        summed = part_own[j, 0] + part_y_far[j, 0].astype(jnp.float32)
        summed = summed + part_z_far[j].astype(jnp.float32)
        out_buf[:, at_cols] = (middle_buf[:, at_cols].astype(jnp.float32) + summed).astype(
            jnp.bfloat16
        )
        put_out(j).start()

    def over_x(what, k):
        def one(i, carry):
            what(k, i)
            return carry

        lax.fori_loop(0, nx, one, 0)

    pl.when(inside_line)(lambda: nears(1, 2))

    def at_ends(k, bs):
        @pl.when(jnp.logical_not(inside_line))
        def _():
            for b in bs:
                relay_near(1, k, b)

    at_ends(3, subs)
    fars(1, 0)
    over_x(lower, 0)
    at_ends(2, subs[:1])
    fars(1, 1)
    lower(1, 0)
    at_ends(2, subs[1:2])
    lower(1, 1)
    over_x(pass_on, 0)
    fars(1, 3)
    at_ends(2, subs[2:3])
    lower(3, 0)
    lower(3, 1)
    over_x(pass_on, 1)
    at_ends(2, subs[3:])
    lower(2, 0)
    for b in subs[:-1]:
        relay_far(1, 2, b)
    over_x(pass_on, 3)
    relay_far(1, 2, SUBS - 1)
    pass_on(2, 0)
    lower(2, 1)
    over_x(finish, 3)
    pass_on(2, 1)
    over_x(finish, 2)
    over_x(finish, 0)
    over_x(finish, 1)

    all_left(7, out_buf)
    all_left(1, up_buf.at[pl.ds(0, nz * nc * depth), :])
    all_left(2, up_buf)
    pl.when(inside_line)(lambda: all_left(0, up_buf.at[pl.ds(0, 8 * depth), :]))
    pl.when(jnp.logical_not(inside_line))(lambda: all_left(0, up_buf.at[pl.ds(0, 4 * depth), :]))
    all_left(3, states.at[pl.ds(0, plane - 1)])
    all_left(4, gathered.at[pl.ds(0, 3 * own), :])
    all_left(5, part_y)
    all_left(6, part_z)
    for copy in [send_wout, pass_wout, send_mixed]:
        copy.wait_send()
    for d in range(1, back + 1):
        pl.when(z + d < nz)(lambda d=d: send_total(d).wait_send())


def fused(
    residual,
    query_vectors,
    key_vectors,
    value_vectors,
    in_gate,
    forget_gate,
    documents,
    w_out,
    norm_gain,
    w_up,
    w_down,
):
    sizes = tuple(lax.axis_size(name) for name in ("z", "x", "c", "tp"))
    nz, nx, nc, ny = sizes
    rows, width = query_vectors.shape
    heads = in_gate.shape[0]
    own, model = residual.shape
    depth, cols = w_up.shape[0], w_down.shape[1]
    units = w_up.shape[1] // PAIR
    members = PAIR * ny
    plane = nx * nc
    pairs = heads // 2
    state = (pairs * (width // heads + 8), width // pairs)
    reach = min(nz * plane - 1, -(-(DOC_MOST - 1) // rows))
    back = -(-reach // plane)
    bf16, f32 = jnp.bfloat16, jnp.float32
    dma = pltpu.SemaphoreType.DMA
    vmem = pl.BlockSpec(memory_space=pltpu.VMEM)
    anywhere = pl.BlockSpec(memory_space=pl.ANY)
    return pl.pallas_call(
        functools.partial(layer_kernel, sizes),
        out_shape=jax.ShapeDtypeStruct((own, model), bf16),
        in_specs=[vmem] * 7 + [anywhere] * 4,
        out_specs=anywhere,
        scratch_shapes=[
            pltpu.VMEM((nz * plane * depth, units), bf16),
            pltpu.VMEM((nz * nx, units, nc * cols), bf16),
            pltpu.VMEM(w_out.shape, bf16),
            pltpu.VMEM(w_out.shape, bf16),
            pltpu.VMEM((own, model), bf16),
            pltpu.VMEM((plane,) + state, f32),
            pltpu.VMEM((1,) + state, f32),
            pltpu.VMEM((back,) + state, f32),
            pltpu.VMEM((rows, width), bf16),
            pltpu.VMEM((own, width), bf16),
            pltpu.VMEM((members * own, model), bf16),
            pltpu.VMEM((members * own, units), bf16),
            pltpu.VMEM((own, model), bf16),
            pltpu.VMEM((nz * nx, PAIR, own, nc * cols), f32),
            pltpu.VMEM((nz * nx, PAIR, own, nc * cols), bf16),
            pltpu.VMEM((nz * nx, PAIR, own, nc * cols), bf16),
            pltpu.VMEM((nz * nx, own, nc * cols), bf16),
            pltpu.VMEM((nz * nx, own, nc * cols), bf16),
            pltpu.VMEM((own, model), bf16),
            dma((2, nz, SUBS)),
            dma((2, nz, SUBS)),
            dma((2, nz, nx)),
            dma((8,)),
            dma((3,)),
            dma((plane,)),
            dma((2, back)),
            dma((2,)),
            dma((4,)),
            dma((3, 2)),
            dma((nz * nx, PAIR)),
            dma((nz * nx,)),
        ],
        compiler_params=pltpu.CompilerParams(
            collective_id=0, has_side_effects=True, vmem_limit_bytes=60 * 1024 * 1024
        ),
    )(
        query_vectors,
        key_vectors,
        value_vectors,
        in_gate,
        forget_gate,
        documents.reshape(1, rows),
        norm_gain,
        residual,
        w_out,
        w_up,
        w_down,
    )


def suits(shape, args):
    nz, nx, nc, ny = shape
    query_vectors, in_gate, w_up, w_down = args[1], args[4], args[9], args[10]
    total, width = query_vectors.shape
    depth, cols = w_up.shape[0] // (nz * nx * nc), w_down.shape[1] // (nz * nx * nc)
    heads = in_gate.shape[0] // ny
    return (
        (nz, nx, nc, ny) == (2 * PAIR, 2, 2, 2)
        and depth % 128 == 0
        and cols % 128 == 0
        and heads == 4
        and width // in_gate.shape[0] == 64
        and total // (nz * nx * nc) == 256
    )


def solution(mesh):
    sp, tp = mesh.shape["sp"], mesh.shape["tp"]
    chips = tp if sp % (2 * tp) == 0 else 1
    cores = 2 if sp % 2 == 0 else 1
    shape = (sp // (chips * cores), chips, cores, tp)
    split = Mesh(np.asarray(mesh.devices).reshape(shape), ("z", "x", "c", "tp"))
    placed = (
        P(("z", "x", "c", "tp"), None),
        P(SP, "tp"),
        P(SP, "tp"),
        P(SP, "tp"),
        P("tp", SP),
        P("tp", SP),
        P(SP),
        P("tp", None),
        P(),
        P(SP, "tp"),
        P("tp", SP),
    )

    def run(*args):
        return jax.shard_map(
            fused if suits(shape, args) else on_device,
            mesh=split,
            in_specs=placed,
            out_specs=P(("z", "x", "c", "tp"), None),
            check_vma=False,
        )(*args)

    return run
```

```python
import functools

import jax
import jax.numpy as jnp
import numpy as np
from jax import lax
from jax.experimental import pallas as pl
from jax.experimental.pallas import tpu as pltpu
from jax.sharding import Mesh, PartitionSpec as P

DOC_MOST = 2048
very_negative = -1e30
epsilon = 1e-06
SP = ("z", "x", "c")
G = ("x", "c")


def combine(earlier, later):
    memory_one, top_one, decay_one, first_one, last_one = earlier
    memory_two, top_two, decay_two, first_two, last_two = later
    later_empty = first_two < 0.0
    earlier_empty = first_one < 0.0
    keep = later_empty | (first_two == last_two) & (first_two == last_one)
    decay_step = jnp.where(later_empty, 0.0, decay_two)
    top_new = jnp.where(keep, jnp.maximum(decay_step + top_one, top_two), top_two)
    scale_old = jnp.where(keep, jnp.exp(decay_step + top_one - top_new), 0.0)
    scale_new = jnp.exp(top_two - top_new)
    memory_new = scale_old[:, None, None] * memory_one + scale_new[:, None, None] * memory_two
    decay_new = jnp.where(keep, decay_one + decay_step, decay_two)
    first_new = jnp.where(earlier_empty, first_two, first_one)
    last_new = jnp.where(later_empty, last_one, last_two)
    return (memory_new, top_new, decay_new, first_new, last_new)


def pack(state):
    memory, top, decay, first, last = state
    heads, _, width = memory.shape
    row = jnp.stack(
        [top, decay, jnp.broadcast_to(first, top.shape), jnp.broadcast_to(last, top.shape)], axis=1
    )
    row = jnp.pad(row, ((0, 0), (0, width - 4)))
    return jnp.concatenate(
        [memory, row[:, None, :], jnp.zeros((heads, 6, width), jnp.float32)], axis=1
    )


def unpack(packed, present):
    rows = packed.shape[1] - 7
    row = packed[:, rows]
    memory = jnp.where(present, packed[:, :rows], 0.0)
    top = jnp.where(present, row[:, 0], very_negative)
    decay = jnp.where(present, row[:, 1], 0.0)
    first = jnp.where(present, row[0, 2], -1.0)
    last = jnp.where(present, row[0, 3], -1.0)
    return (memory, top, decay, first, last)


def shifted(state, distance, length, here):
    packed = lax.ppermute(pack(state), SP, [(i, i + distance) for i in range(length - distance)])
    return unpack(packed, here >= distance)


def turn(value, axis, d):
    n = lax.axis_size(axis)
    return lax.ppermute(value, axis, [(i, (i + d) % n) for i in range(n)])


def reduced(terms, dim, axis):
    def block(d):
        return lax.index_in_dim(terms, d, dim, keepdims=False)

    total = block(0).astype(jnp.float32)
    for d in range(1, lax.axis_size(axis)):
        total = total + turn(block(d), axis, -d).astype(jnp.float32)
    return total.astype(jnp.bfloat16)


def on_device(
    residual,
    query_vectors,
    key_vectors,
    value_vectors,
    in_gate,
    forget_gate,
    documents,
    w_out,
    norm_gain,
    w_up,
    w_down,
):
    tok_rows = query_vectors.shape[0]
    heads = in_gate.shape[0]
    head_dim = query_vectors.shape[1] // heads
    length = lax.axis_size(SP)
    here = lax.axis_index(SP)
    tp = lax.axis_size("tp")
    me = lax.axis_index("tp")

    plane = lax.axis_size(G)
    up_pieces = jnp.transpose(w_up.reshape(w_up.shape[0], plane, -1), (1, 0, 2))
    up_part = lax.all_to_all(up_pieces, G, split_axis=0, concat_axis=0, tiled=True)
    up_part = up_part.reshape(-1, up_part.shape[-1])
    up_part, w_down, w_out, key_vectors, in_gate, forget_gate, documents = (
        lax.optimization_barrier(
            (up_part, w_down, w_out, key_vectors, in_gate, forget_gate, documents)
        )
    )
    down_part = lax.all_to_all(w_down, G, split_axis=0, concat_axis=1, tiled=True)
    up_all = lax.all_gather(up_part, "z", axis=0, tiled=True)
    down_all = lax.all_gather(down_part, "z", axis=1, tiled=True)

    w_out_parts = [w_out] + [turn(w_out, "tp", d) for d in range(1, tp)]

    segment = documents.astype(jnp.float32)
    decay_log = jax.nn.log_sigmoid(forget_gate)
    cumulative = jnp.cumsum(decay_log, axis=-1)
    key_heads = jnp.transpose(key_vectors.reshape(tok_rows, heads, head_dim), (1, 0, 2))
    value_heads = jnp.transpose(value_vectors.reshape(tok_rows, heads, head_dim), (1, 0, 2))
    query_heads = jnp.transpose(query_vectors.reshape(tok_rows, heads, head_dim), (1, 0, 2))
    query_heads = query_heads * jnp.asarray(head_dim ** (-0.5), query_heads.dtype)
    latest = segment == segment[-1]
    growth = jnp.where(latest[None, :], cumulative[:, -1:] - cumulative + in_gate, very_negative)
    top_log = jnp.max(growth, axis=-1)
    summary_weight = jnp.exp(growth - top_log[:, None])
    key_wide = key_heads.astype(jnp.float32)
    weighted = key_wide * summary_weight[:, :, None]
    memory = jnp.einsum(
        "hsv,hsk->hvk", value_heads.astype(jnp.float32), weighted, precision=lax.Precision.HIGHEST
    )
    normal = jnp.sum(weighted, axis=1)
    state = (
        jnp.concatenate([memory, normal[:, None, :]], axis=1),
        top_log,
        cumulative[:, -1],
        segment[0],
        segment[-1],
    )

    reach = min(length - 1, -(-(DOC_MOST - 1) // tok_rows))
    span = 1
    while span < reach:
        state = combine(shifted(state, span, length, here), state)
        span *= 2
    incoming = shifted(state, 1, length, here)
    memory_in, top_in, _, _, last_in = incoming

    row_ids = lax.broadcasted_iota(jnp.int32, (tok_rows, tok_rows), 0)
    col_ids = lax.broadcasted_iota(jnp.int32, (tok_rows, tok_rows), 1)
    allowed = (col_ids <= row_ids) & (segment[:, None] == segment[None, :])
    inside = jnp.where(
        allowed[None],
        cumulative[:, :, None] - cumulative[:, None, :] + in_gate[:, None, :],
        very_negative,
    )
    peak_inside = jnp.max(inside, axis=-1)
    scores = jnp.einsum(
        "hld,hsd->hls", query_heads, key_heads, preferred_element_type=jnp.float32
    )
    weight_inside = jnp.exp(inside - peak_inside[:, :, None]) * scores
    from_block = jnp.einsum(
        "hls,hsv->hlv",
        weight_inside.astype(jnp.bfloat16),
        value_heads,
        preferred_element_type=jnp.float32,
    )
    sum_inside = jnp.sum(weight_inside, axis=-1)

    outside = jnp.where((segment == last_in)[None, :], cumulative + top_in[:, None], very_negative)
    peak_log = jnp.maximum(outside, peak_inside)
    carried = jnp.exp(outside - peak_log)
    local = jnp.exp(peak_inside - peak_log)
    readout = jnp.einsum(
        "hlk,hvk->hlv",
        query_heads.astype(jnp.float32),
        memory_in,
        precision=lax.Precision.HIGHEST,
    )
    numer = carried[:, :, None] * readout[:, :, :head_dim] + local[:, :, None] * from_block
    denom = carried * readout[:, :, head_dim] + local * sum_inside
    mixed = numer / jnp.maximum(jnp.abs(denom), jnp.exp(-peak_log))[:, :, None]
    mixed = jnp.transpose(mixed, (1, 0, 2)).reshape(tok_rows, -1).astype(jnp.bfloat16)

    own_rows = tok_rows // tp
    mixed_rows = mixed.reshape(tp, own_rows, -1)
    projected = 0.0
    for d in range(tp):
        piece = lax.dynamic_index_in_dim(mixed_rows, (me + d) % tp, 0, keepdims=False)
        if d:
            piece = turn(piece, "tp", d)
        projected = projected + jnp.dot(
            piece, w_out_parts[d], preferred_element_type=jnp.float32
        )
    middle = (residual.astype(jnp.float32) + projected).astype(jnp.bfloat16)
    middle_wide = middle.astype(jnp.float32)
    factor = lax.rsqrt(jnp.mean(middle_wide * middle_wide, axis=-1, keepdims=True) + epsilon)
    normed = (middle_wide * factor * norm_gain.astype(jnp.float32)).astype(jnp.bfloat16)

    gathered = normed
    for axis in ("tp", "x", "c"):
        gathered = jnp.concatenate(
            [gathered] + [turn(gathered, axis, d) for d in range(1, lax.axis_size(axis))], axis=0
        )
    lifted = jnp.dot(gathered, up_all, preferred_element_type=jnp.float32)
    hidden = jnp.square(jax.nn.relu(lifted)).astype(jnp.bfloat16)
    sizes = (lax.axis_size("c"), lax.axis_size("x"), tp)
    half = down_all.shape[1] // 2
    summed = []
    for k, order in enumerate((("c", "x", "tp"), ("c", "tp", "x"))):
        terms = jnp.dot(
            hidden, down_all[:, k * half : (k + 1) * half], preferred_element_type=jnp.float32
        )
        terms = terms.astype(jnp.bfloat16).reshape(*sizes, own_rows, half)
        names = ["c", "x", "tp"]
        for axis in order:
            terms = reduced(terms, names.index(axis), axis)
            names.remove(axis)
        summed.append(terms.astype(jnp.float32))
    return (middle_wide + jnp.concatenate(summed, axis=1)).astype(jnp.bfloat16)


MESH = pl.DeviceIdType.MESH
PAIR = 2
SUBS = 4
NT = (((1,), (1,)), ((), ()))
NN = (((1,), (0,)), ((), ()))


def dot(a, b, dims=NN):
    return lax.dot_general(a, b, dims, preferred_element_type=jnp.float32)


def thirds(value):
    high = value.astype(jnp.bfloat16)
    rest = value - high.astype(jnp.float32)
    middle = rest.astype(jnp.bfloat16)
    low = (rest - middle.astype(jnp.float32)).astype(jnp.bfloat16)
    return high, middle, low


def combine_rows(earlier, later):
    memory_one, normal_one, top_one, decay_one, first_one, last_one = earlier
    memory_two, normal_two, top_two, decay_two, first_two, last_two = later
    later_empty = first_two < 0.0
    earlier_empty = first_one < 0.0
    keep = later_empty | (first_two == last_two) & (first_two == last_one)
    decay_step = jnp.where(later_empty, 0.0, decay_two)
    top_new = jnp.where(keep, jnp.maximum(decay_step + top_one, top_two), top_two)
    scale_old = jnp.where(keep, jnp.exp(decay_step + top_one - top_new), 0.0)
    scale_new = jnp.exp(top_two - top_new)
    return (
        scale_old * memory_one + scale_new * memory_two,
        scale_old * normal_one + scale_new * normal_two,
        top_new,
        jnp.where(keep, decay_one + decay_step, decay_two),
        jnp.where(earlier_empty, first_two, first_one),
        jnp.where(later_empty, last_one, last_two),
    )


def choose(flag, one, two):
    return tuple(jnp.where(flag, a, b) for a, b in zip(one, two))


def layer_kernel(
    sizes,
    query_ref,
    key_ref,
    value_ref,
    in_ref,
    forget_ref,
    document_ref,
    gain_ref,
    residual_ref,
    w_out_ref,
    w_up_ref,
    w_down_ref,
    out_ref,
    up_buf,
    down_buf,
    wout_own,
    wout_far,
    residual_buf,
    states,
    totals,
    before,
    mixed_buf,
    mixed_far,
    gathered,
    hidden,
    middle_buf,
    part_own,
    part_y,
    part_y_far,
    part_z,
    part_z_far,
    out_buf,
    line_sem,
    far_sem,
    core_sem,
    sent,
    local_sem,
    state_sem,
    total_sem,
    mix_sem,
    wout_sem,
    gather_sem,
    part_y_sem,
    part_z_sem,
):
    nz, nx, nc, ny = sizes
    z, x, c, y = (lax.axis_index(name) for name in ("z", "x", "c", "tp"))
    zl = z // PAIR
    zn = lax.rem(z + PAIR, nz)
    rows, width = query_ref.shape
    heads = in_ref.shape[0]
    pairs = heads // 2
    lanes = width // pairs
    hd = lanes // 2
    own = rows // ny
    model = out_ref.shape[1]
    depth = w_up_ref.shape[0]
    cols = w_down_ref.shape[1]
    units = w_up_ref.shape[1] // PAIR
    sub = units // SUBS
    plane = nx * nc
    spot = x * nc + c
    tile = nc * cols

    def remote(src, dst, send, recv, dev):
        return pltpu.make_async_remote_copy(
            src_ref=src,
            dst_ref=dst,
            send_sem=send,
            recv_sem=recv,
            device_id=dev,
            device_id_type=MESH,
        )

    x_dev = (z, 1 - x, c, y)
    c_dev = (z, x, 1 - c, y)
    y_dev = (z, x, c, 1 - y)
    n_dev = (zn, x, c, y)

    def place(s, xx, cc):
        return (s * nx + xx) * nc + cc

    def slot(m, s, xx, cc, b):
        if m == 0:
            start = pl.multiple_of(place(s, xx, cc) * depth, depth)
            return up_buf.at[pl.ds(start, depth), pl.ds(b * sub, sub)]
        lane0 = pl.multiple_of(cc * cols, cols)
        return down_buf.at[s * nx + xx, pl.ds(b * sub, sub), pl.ds(lane0, cols)]

    def source(m, g, b):
        start = pl.multiple_of(g * units + b * sub, sub)
        if m == 0:
            return w_up_ref.at[:, pl.ds(start, sub)]
        return w_down_ref.at[pl.ds(start, sub), :]

    def send_z(m, g, s, to, b):
        src = source(m, g, b) if s is None else slot(m, s, x, c, b)
        s = z if s is None else s
        return remote(
            src,
            slot(m, s, x, c, b),
            sent.at[0],
            line_sem.at[m, s, b],
            (jnp.int32(to), x, c, y),
        )

    def send_x(m, k, s, b):
        src = source(m, zl, b) if k == 0 else slot(m, s, x, c, b)
        return remote(src, slot(m, s, x, c, b), sent.at[1], far_sem.at[m, s, b], x_dev)

    def send_c(m, k, s, far, b):
        xx = 1 - x if far else x
        src = source(m, zl, b) if k == 0 and not far else slot(m, s, xx, c, b)
        return remote(src, slot(m, s, xx, c, b), sent.at[2], core_sem.at[m, s, xx], c_dev)

    def arrived(m, s, xx, b, sem):
        here = slot(m, s, xx, c, b)
        remote(here, here, sent.at[1], sem.at[m, s, b], x_dev).wait_recv()

    def shared(m, s, xx):
        start = pl.multiple_of(place(s, xx, 1 - c) * depth, depth)
        lane0 = pl.multiple_of((1 - c) * cols, cols)
        here = (
            up_buf.at[pl.ds(start, depth), :],
            down_buf.at[s * nx + xx, :, pl.ds(lane0, cols)],
        )[m]
        remote(here, here, sent.at[2], core_sem.at[m, s, xx], c_dev).wait_recv()

    def local(m, b):
        return pltpu.make_async_copy(source(m, zl, b), slot(m, z, x, c, b), local_sem.at[0])

    def all_left(kind, like):
        pltpu.make_async_copy(like, like, sent.at[kind]).wait()

    to_left = {1: [(0, 0)], 2: [(0, 1)], 3: [(1, 2), (0, 1)]}
    to_right = {0: [(0, 1), (1, 2)], 1: [(1, 2)], 2: [(1, 3)]}

    def on_line(m, places, act, late=(False, True)):
        for kz in places:
            lefts, rights = to_left.get(kz, []), to_right.get(kz, [])
            todo = []
            for i, (g, to) in enumerate(lefts + rights):
                for b in range(SUBS):
                    behind = i > len(lefts) or (i == len(lefts) and b >= ahead[kz])
                    if behind in late:
                        todo.append((i, g, to, b))

            @pl.when(z == kz)
            def _(todo=todo):
                for i, g, to, b in todo:
                    act(send_z(m, g, None, to, b))

    ends, mids = (0, nz - 1), tuple(range(1, nz - 1))
    ahead = (1, 2, 2, 0)
    inside_line = (z > 0) & (z < nz - 1)

    def on_relay(m, k, b, act):
        for kz, to in ((1, 0), (2, 3)):
            pl.when(z == kz)(lambda to=to: act(send_z(m, None, order[k], to, b)))

    start = lambda copy: copy.start()
    order = [z, z + 1 - 2 * lax.rem(z, PAIR), 2 - z // 2, (nz - 1) * (1 - z // 2)]

    barrier = pltpu.get_barrier_semaphore()
    partners = [(lax.rem(z + d, nz), x, c, y) for d in range(1, nz)]
    partners += [x_dev, c_dev, (z, 1 - x, 1 - c, y), y_dev]
    for dev in partners:
        pl.semaphore_signal(barrier, inc=1, device_id=dev, device_id_type=MESH)

    load_residual = pltpu.make_async_copy(residual_ref, residual_buf, local_sem.at[1])
    load_wout = pltpu.make_async_copy(w_out_ref, wout_own, local_sem.at[2])
    load_residual.start()
    load_wout.start()
    for m in range(2):
        for b in range(SUBS):
            local(m, b).start()

    near = lax.broadcasted_iota(jnp.int32, (1, lanes), 1) < hd
    forget = forget_ref[...]
    decay_log = jnp.minimum(forget, 0.0) - jnp.log1p(jnp.exp(-jnp.abs(forget)))
    gates = jnp.concatenate([decay_log, in_ref[...]], axis=0)
    at = lax.broadcasted_iota(jnp.int32, gates.shape, 1)
    running = gates
    step = 1
    while step < rows:
        running = running + jnp.where(at >= step, pltpu.roll(running, step, 1), 0.0)
        step *= 2
    cum_row = running[:heads]
    in_row = gates[heads:]
    seg_row = document_ref[...].astype(jnp.float32)
    seg_first = seg_row[:, 0:1]
    seg_last = seg_row[:, rows - 1 : rows]
    total = cum_row[:, rows - 1 : rows]
    growth = jnp.where(seg_row == seg_last, total - cum_row + in_row, very_negative)
    top = jnp.max(growth, axis=1, keepdims=True)
    summary = jnp.exp(growth - top)
    columns = jnp.transpose(jnp.concatenate([summary, cum_row], axis=0))
    seg_col = jnp.transpose(jnp.broadcast_to(seg_row, (2 * heads, rows)))[:, 0:1]

    row_of = lax.broadcasted_iota(jnp.int32, (8, lanes), 0)
    tall = hd + 8

    def store(ref, i, p, state):
        info = jnp.zeros((8, lanes), jnp.float32)
        for j, line in enumerate(state[1:]):
            info = jnp.where(row_of == j, line, info)
        ref[i, p * tall : p * tall + hd, :] = state[0]
        ref[i, p * tall + hd : (p + 1) * tall, :] = info

    for p in range(pairs):
        a, b = 2 * p, 2 * p + 1
        span = pl.ds(p * lanes, lanes)
        keys = key_ref[:, span].astype(jnp.float32)
        weighted = keys * jnp.where(near, columns[:, a : a + 1], columns[:, b : b + 1])
        values_t = jnp.transpose(value_ref[:, span])
        full = sum(dot(values_t, piece) for piece in thirds(weighted))
        memory = jnp.where(near, full[:hd], full[hd:])
        normal = jnp.sum(weighted, axis=0, keepdims=True)
        top_row = jnp.where(near, top[a : a + 1], top[b : b + 1])
        decay_row = jnp.where(near, total[a : a + 1], total[b : b + 1])
        store(states, spot, p, (memory, normal, top_row, decay_row, seg_first, seg_last))

    def send_state(i, dev):
        return remote(states.at[i], states.at[i], sent.at[3], state_sem.at[i], dev)

    pl.semaphore_wait(barrier, len(partners))

    beside, across = spot + 1 - 2 * c, (1 - x) * nc + c
    send_state(spot, x_dev).start()
    send_state(spot, c_dev).start()
    on_line(0, range(nz), start, late=(False,))
    half = wout_far.shape[0] // nc

    def wout_rows(cc):
        return pl.ds(pl.multiple_of(cc * half, half), half)

    send_wout = remote(
        w_out_ref.at[wout_rows(c)], wout_far.at[wout_rows(c)], wout_sem.at[0], wout_sem.at[1], y_dev
    )
    pass_wout = remote(
        wout_far.at[wout_rows(c)], wout_far.at[wout_rows(c)], wout_sem.at[2], wout_sem.at[3], c_dev
    )
    send_wout.start()
    for b in range(SUBS):
        send_c(0, 0, z, False, b).start()
    for b in range(SUBS):
        send_x(0, 0, z, b).start()
    send_x(1, 0, z, 0).start()

    row_ids = lax.broadcasted_iota(jnp.int32, (rows, rows), 0)
    col_ids = lax.broadcasted_iota(jnp.int32, (rows, rows), 1)
    allowed = (col_ids <= row_ids) & (seg_col == seg_row)
    inner = []
    for p in range(pairs):
        span = pl.ds(p * lanes, lanes)
        queries = query_ref[:, span] * jnp.asarray(hd**-0.5, jnp.bfloat16)
        keys = key_ref[:, span]
        values = value_ref[:, span]
        zero = jnp.zeros_like(queries)
        peaks, sums, outs = [], [], []
        for i in range(2):
            h = 2 * p + i
            mine = near if i == 0 else jnp.logical_not(near)
            scores = dot(jnp.where(mine, queries, zero), keys, NT)
            cum_col = columns[:, heads + h : heads + h + 1]
            inside = jnp.where(
                allowed, cum_col - cum_row[h : h + 1] + in_row[h : h + 1], very_negative
            )
            peak = jnp.max(inside, axis=1, keepdims=True)
            weight = jnp.exp(inside - peak) * scores
            peaks.append(peak)
            sums.append(jnp.sum(weight, axis=1, keepdims=True))
            outs.append(dot(weight.astype(jnp.bfloat16), jnp.where(mine, values, zero)))
        cum_pair = jnp.where(
            near,
            columns[:, heads + 2 * p : heads + 2 * p + 1],
            columns[:, heads + 2 * p + 1 : heads + 2 * p + 2],
        )
        inner.append(
            (
                queries,
                cum_pair,
                jnp.where(near, peaks[0], peaks[1]),
                jnp.where(near, sums[0], sums[1]),
                outs[0] + outs[1],
            )
        )

    def load(ref, i, p):
        info = ref[i, p * tall + hd : (p + 1) * tall, :]
        return (ref[i, p * tall : p * tall + hd, :],) + tuple(info[j : j + 1] for j in range(5))

    def empty():
        zero = jnp.zeros((1, lanes), jnp.float32)
        return (
            jnp.zeros((hd, lanes), jnp.float32),
            zero,
            zero + very_negative,
            zero,
            zero - 1.0,
            zero - 1.0,
        )

    send_state(across, x_dev).wait_recv()
    send_state(across, c_dev).start()
    send_state(beside, c_dev).wait_recv()
    send_state(across + 1 - 2 * c, c_dev).wait_recv()
    prefix = []
    for p in range(pairs):
        so_far = load(states, 0, p)
        mine = choose(spot == 0, empty(), so_far)
        for i in range(1, plane):
            if i > 1:
                mine = choose(spot == i, so_far, mine)
            so_far = combine_rows(so_far, load(states, i, p))
        prefix.append(mine)
        store(totals, 0, p, so_far)

    back = before.shape[0]

    def send_total(d):
        return remote(
            totals.at[0],
            before.at[d - 1],
            total_sem.at[0, d - 1],
            total_sem.at[1, d - 1],
            (lax.rem(z + d, nz), x, c, y),
        )

    for d in range(back, 0, -1):
        pl.when(z + d < nz)(lambda d=d: send_total(d).start())
    on_line(0, range(nz), start, late=(True,))

    for d in range(1, back + 1):
        pl.when(z >= d)(lambda d=d: send_total(d).wait_recv())

        @pl.when(z < d)
        def _(d=d):
            for p in range(pairs):
                store(before, d - 1, p, empty())

    wide_near = lax.broadcasted_iota(jnp.int32, (lanes, lanes), 1) < hd
    wide_top = lax.broadcasted_iota(jnp.int32, (lanes, lanes), 0) < hd
    block = wide_near == wide_top
    for p in range(pairs):
        queries, cum_pair, peak_in, sum_in, from_block = inner[p]
        incoming = load(before, back - 1, p)
        for d in range(back - 1, 0, -1):
            incoming = combine_rows(incoming, load(before, d - 1, p))
        memory, normal, top_row, _, _, last_row = combine_rows(incoming, prefix[p])
        outside = jnp.where(seg_col == last_row, cum_pair + top_row, very_negative)
        peak = jnp.maximum(outside, peak_in)
        carried = jnp.exp(outside - peak)
        inside = jnp.exp(peak_in - peak)
        keep = jnp.where(block, jnp.concatenate([memory, memory], axis=0), 0.0)
        norms = jnp.where(block, jnp.broadcast_to(normal, (lanes, lanes)), 0.0)
        both = jnp.concatenate([keep, norms], axis=0)
        readout = sum(dot(queries, piece, NT) for piece in thirds(both))
        numer = carried * readout[:, :lanes] + inside * from_block
        denom = carried * readout[:, lanes:] + inside * sum_in
        mixed = numer / jnp.maximum(jnp.abs(denom), jnp.exp(-peak))
        mixed_buf[:, p * lanes : (p + 1) * lanes] = mixed.astype(jnp.bfloat16)

    far_rows = pl.ds(pl.multiple_of((1 - y) * own, own), own)
    own_rows = pl.ds(pl.multiple_of(y * own, own), own)
    send_mixed = remote(mixed_buf.at[far_rows], mixed_far, mix_sem.at[0], mix_sem.at[1], y_dev)
    send_mixed.start()

    def relay_near(m, k, b):
        arrived(m, order[k], x, b, line_sem)
        if k > 1:
            on_relay(m, k, b, start)
        send_x(m, k, order[k], b).start()
        send_c(m, k, order[k], False, b).start()

    def relay_far(m, k, b):
        arrived(m, order[k], 1 - x, b, far_sem)
        send_c(m, k, order[k], True, b).start()

    subs = range(SUBS)
    @pl.when(inside_line)
    def _():
        for b in subs[:2]:
            relay_near(0, 2, b)

    load_residual.wait()
    load_wout.wait()
    projected = dot(mixed_buf[own_rows, :], wout_own[...])
    send_wout.wait_recv()
    pass_wout.start()
    send_mixed.wait_recv()
    remote(
        wout_far.at[wout_rows(1 - c)],
        wout_far.at[wout_rows(1 - c)],
        wout_sem.at[2],
        wout_sem.at[3],
        c_dev,
    ).wait_recv()
    projected = projected + dot(mixed_far[...], wout_far[...])
    middle = (residual_buf[...].astype(jnp.float32) + projected).astype(jnp.bfloat16)
    middle_buf[...] = middle
    wide = middle.astype(jnp.float32)
    factor = lax.rsqrt(jnp.mean(wide * wide, axis=-1, keepdims=True) + epsilon)
    gain = gain_ref[...].astype(jnp.float32).reshape(1, model)
    gathered[0:own, :] = (wide * factor * gain).astype(jnp.bfloat16)

    part = own // 2

    def give(kind, h):
        src, dst, dev = ((0, 2, n_dev), (0, 1, y_dev), (2, 3, y_dev))[kind]
        return remote(
            gathered.at[pl.ds(src * own + h * part, part)],
            gathered.at[pl.ds(dst * own + h * part, part)],
            sent.at[4],
            gather_sem.at[dst - 1, h],
            dev,
        )

    for h in range(2):
        give(0, h).start()
    for h in range(2):
        give(1, h).start()

    def take(h):
        give(0, h).wait_recv()
        give(2, h).start()

    for b in subs:
        relay_near(0, 1, b)
    pl.when(jnp.logical_not(inside_line))(lambda: [relay_near(0, 2, b) for b in subs[:2]] and None)
    for b in subs[2:-1]:
        relay_near(0, 2, b)
    on_line(1, ends, start)
    for b in subs:
        send_c(1, 0, z, False, b).start()
    for b in range(1, SUBS):
        send_x(1, 0, z, b).start()
    for b in subs:
        relay_near(0, nz - 1, b)
    relay_near(0, 2, SUBS - 1)
    for h in range(2):
        take(h)
    on_line(1, mids, start)
    def nears(m, k):
        for b in subs:
            relay_near(m, k, b)

    def fars(m, k):
        for b in subs:
            relay_far(m, k, b)

    for k in range(nz - 1):
        fars(0, k)
    nears(1, 1)
    @pl.when(inside_line)
    def _():
        for b in subs[:-1]:
            relay_near(1, 3, b)

    fars(0, nz - 1)

    here = up_buf.at[pl.ds(0, 2 * depth), :]
    pltpu.make_async_copy(here, here, local_sem.at[0]).wait()
    for s in order:
        for xx in range(nx):
            shared(0, s, lax.rem(x + xx, nx))
    for h in range(2):
        give(1, h).wait_recv()
        give(2, h).wait_recv()

    pl.when(inside_line)(lambda: relay_near(1, 3, SUBS - 1))
    def lift(i, carry):
        at_units = pl.ds(pl.multiple_of(i * tile, tile), tile)
        lifted = dot(gathered[...], up_buf[:, at_units])
        positive = jnp.maximum(lifted, 0.0)
        hidden[:, at_units] = (positive * positive).astype(jnp.bfloat16)
        return carry

    lax.fori_loop(0, units // tile, lift, 0)

    def send_part_y(j, dz):
        return remote(
            part_y.at[j, dz], part_y_far.at[j, dz], sent.at[5], part_y_sem.at[j, dz], y_dev
        )

    def send_part_z(j):
        return remote(part_z.at[j], part_z_far.at[j], sent.at[6], part_z_sem.at[j], n_dev)

    def lower(k, dx):
        s, xx = order[k], lax.rem(x + dx, nx)
        j = s * nx + xx
        shared(1, s, xx)
        terms = dot(hidden[...], down_buf[j])
        for dz in reversed(range(PAIR)):
            first = dz * ny * own
            part_own[j, dz] = terms[first : first + own]
            part_y[j, dz] = terms[first + own : first + 2 * own].astype(jnp.bfloat16)
        for dz in reversed(range(PAIR)):
            send_part_y(j, dz).start()

    def pass_on(k, dx):
        j = order[k] * nx + lax.rem(x + dx, nx)
        send_part_y(j, 1).wait_recv()
        summed = part_own[j, 1] + part_y_far[j, 1].astype(jnp.float32)
        part_z[j] = summed.astype(jnp.bfloat16)
        send_part_z(j).start()

    def put_out(j):
        at_cols = pl.ds(pl.multiple_of(j * tile, tile), tile)
        return pltpu.make_async_copy(out_buf.at[:, at_cols], out_ref.at[:, at_cols], sent.at[7])

    def finish(k, dx):
        j = order[k] * nx + lax.rem(x + dx, nx)
        send_part_y(j, 0).wait_recv()
        send_part_z(j).wait_recv()
        at_cols = pl.ds(pl.multiple_of(j * tile, tile), tile)
        summed = part_own[j, 0] + part_y_far[j, 0].astype(jnp.float32)
        summed = summed + part_z_far[j].astype(jnp.float32)
        out_buf[:, at_cols] = (middle_buf[:, at_cols].astype(jnp.float32) + summed).astype(
            jnp.bfloat16
        )
        put_out(j).start()

    def over_x(what, k):
        def one(i, carry):
            what(k, i)
            return carry

        lax.fori_loop(0, nx, one, 0)

    pl.when(inside_line)(lambda: nears(1, 2))

    def at_ends(k, bs):
        @pl.when(jnp.logical_not(inside_line))
        def _():
            for b in bs:
                relay_near(1, k, b)

    at_ends(3, subs)
    fars(1, 0)
    over_x(lower, 0)
    at_ends(2, subs[:1])
    fars(1, 1)
    lower(1, 0)
    at_ends(2, subs[1:2])
    lower(1, 1)
    over_x(pass_on, 0)
    lower(3, 0)
    over_x(pass_on, 1)
    fars(1, 3)
    at_ends(2, subs[2:3])
    lower(3, 1)
    at_ends(2, subs[3:])
    lower(2, 0)
    pass_on(3, 0)
    for b in subs[:-1]:
        relay_far(1, 2, b)
    pass_on(3, 1)
    relay_far(1, 2, SUBS - 1)
    pass_on(2, 0)
    lower(2, 1)
    over_x(finish, 3)
    pass_on(2, 1)
    over_x(finish, 2)
    over_x(finish, 0)
    over_x(finish, 1)

    all_left(7, out_buf)
    all_left(1, up_buf.at[pl.ds(0, nz * nc * depth), :])
    all_left(2, up_buf)
    pl.when(inside_line)(lambda: all_left(0, up_buf.at[pl.ds(0, 8 * depth), :]))
    pl.when(jnp.logical_not(inside_line))(lambda: all_left(0, up_buf.at[pl.ds(0, 4 * depth), :]))
    all_left(3, states.at[pl.ds(0, plane - 1)])
    all_left(4, gathered.at[pl.ds(0, 3 * own), :])
    all_left(5, part_y)
    all_left(6, part_z)
    for copy in [send_wout, pass_wout, send_mixed]:
        copy.wait_send()
    for d in range(1, back + 1):
        pl.when(z + d < nz)(lambda d=d: send_total(d).wait_send())


def fused(
    residual,
    query_vectors,
    key_vectors,
    value_vectors,
    in_gate,
    forget_gate,
    documents,
    w_out,
    norm_gain,
    w_up,
    w_down,
):
    sizes = tuple(lax.axis_size(name) for name in ("z", "x", "c", "tp"))
    nz, nx, nc, ny = sizes
    rows, width = query_vectors.shape
    heads = in_gate.shape[0]
    own, model = residual.shape
    depth, cols = w_up.shape[0], w_down.shape[1]
    units = w_up.shape[1] // PAIR
    members = PAIR * ny
    plane = nx * nc
    pairs = heads // 2
    state = (pairs * (width // heads + 8), width // pairs)
    reach = min(nz * plane - 1, -(-(DOC_MOST - 1) // rows))
    back = -(-reach // plane)
    bf16, f32 = jnp.bfloat16, jnp.float32
    dma = pltpu.SemaphoreType.DMA
    vmem = pl.BlockSpec(memory_space=pltpu.VMEM)
    anywhere = pl.BlockSpec(memory_space=pl.ANY)
    return pl.pallas_call(
        functools.partial(layer_kernel, sizes),
        out_shape=jax.ShapeDtypeStruct((own, model), bf16),
        in_specs=[vmem] * 7 + [anywhere] * 4,
        out_specs=anywhere,
        scratch_shapes=[
            pltpu.VMEM((nz * plane * depth, units), bf16),
            pltpu.VMEM((nz * nx, units, nc * cols), bf16),
            pltpu.VMEM(w_out.shape, bf16),
            pltpu.VMEM(w_out.shape, bf16),
            pltpu.VMEM((own, model), bf16),
            pltpu.VMEM((plane,) + state, f32),
            pltpu.VMEM((1,) + state, f32),
            pltpu.VMEM((back,) + state, f32),
            pltpu.VMEM((rows, width), bf16),
            pltpu.VMEM((own, width), bf16),
            pltpu.VMEM((members * own, model), bf16),
            pltpu.VMEM((members * own, units), bf16),
            pltpu.VMEM((own, model), bf16),
            pltpu.VMEM((nz * nx, PAIR, own, nc * cols), f32),
            pltpu.VMEM((nz * nx, PAIR, own, nc * cols), bf16),
            pltpu.VMEM((nz * nx, PAIR, own, nc * cols), bf16),
            pltpu.VMEM((nz * nx, own, nc * cols), bf16),
            pltpu.VMEM((nz * nx, own, nc * cols), bf16),
            pltpu.VMEM((own, model), bf16),
            dma((2, nz, SUBS)),
            dma((2, nz, SUBS)),
            dma((2, nz, nx)),
            dma((8,)),
            dma((3,)),
            dma((plane,)),
            dma((2, back)),
            dma((2,)),
            dma((4,)),
            dma((3, 2)),
            dma((nz * nx, PAIR)),
            dma((nz * nx,)),
        ],
        compiler_params=pltpu.CompilerParams(
            collective_id=0, has_side_effects=True, vmem_limit_bytes=60 * 1024 * 1024
        ),
    )(
        query_vectors,
        key_vectors,
        value_vectors,
        in_gate,
        forget_gate,
        documents.reshape(1, rows),
        norm_gain,
        residual,
        w_out,
        w_up,
        w_down,
    )


def suits(shape, args):
    nz, nx, nc, ny = shape
    query_vectors, in_gate, w_up, w_down = args[1], args[4], args[9], args[10]
    total, width = query_vectors.shape
    depth, cols = w_up.shape[0] // (nz * nx * nc), w_down.shape[1] // (nz * nx * nc)
    heads = in_gate.shape[0] // ny
    return (
        (nz, nx, nc, ny) == (2 * PAIR, 2, 2, 2)
        and depth % 128 == 0
        and cols % 128 == 0
        and heads == 4
        and width // in_gate.shape[0] == 64
        and total // (nz * nx * nc) == 256
    )


def solution(mesh):
    sp, tp = mesh.shape["sp"], mesh.shape["tp"]
    chips = tp if sp % (2 * tp) == 0 else 1
    cores = 2 if sp % 2 == 0 else 1
    shape = (sp // (chips * cores), chips, cores, tp)
    split = Mesh(np.asarray(mesh.devices).reshape(shape), ("z", "x", "c", "tp"))
    placed = (
        P(("z", "x", "c", "tp"), None),
        P(SP, "tp"),
        P(SP, "tp"),
        P(SP, "tp"),
        P("tp", SP),
        P("tp", SP),
        P(SP),
        P("tp", None),
        P(),
        P(SP, "tp"),
        P("tp", SP),
    )

    def run(*args):
        return jax.shard_map(
            fused if suits(shape, args) else on_device,
            mesh=split,
            in_specs=placed,
            out_specs=P(("z", "x", "c", "tp"), None),
            check_vma=False,
        )(*args)

    return run
```
